32 devices in a mesh: sp: 16 (over z, y, x), tp: 2 (over core).
Axes of the slice: x: 2, y: 2, z: 4, core: 2. Of those that a mesh axis runs over, the one named last changes fastest.
Arguments:
- residual: bfloat16 [6144, 2048], P('sp'), may hold values from -6 to 6
- queries: bfloat16 [6144, 2048], P('sp', 'tp'), may hold values from -48 to 48
- keys: bfloat16 [6144, 2048], P('sp', 'tp'), may hold values from -48 to 48
- values: bfloat16 [6144, 2048], P('sp', 'tp'), may hold values from -6 to 6
- gate_cache: float32 [6144, 32], P('sp', 'tp'), may hold values from -1544 to 0, as said below
- doc_ids: int32 [6144], P('sp'), may hold values from 0 to 7, never falling along the last dimension, each value on 1 to 1536 neighbouring positions
- out_weight: bfloat16 [2048, 2048], P('tp'), may hold values from -1 to 1
- mix_gain: float32 [2048], replicated, may hold values from 0.1 to 1.9
- gate_weight: bfloat16 [2048, 5120], P('sp', 'tp'), may hold values from -0.125 to 0.125
- up_weight: bfloat16 [2048, 5120], P('sp', 'tp'), may hold values from -0.125 to 0.125
- down_weight: bfloat16 [5120, 2048], P('tp', 'sp'), may hold values from -0.15625 to 0.15625
Outputs:
- layer_out: bfloat16 [6144, 2048], P(('sp', 'tp'))
The draws below stay inside these ranges and needn't reach their ends.
Inputs may be any that keep to these rules, and one draw needn't show every extreme that they name: `doc_ids`: positions of one document are consecutive; each document has 1 to 1536 positions, and one has exactly that many. `gate_cache`: no column rises from one position to the next.
All inputs are finite; a program needn't handle non-finite values.
Results may differ from the reference program's by a relative error of at most 0.018.
Values may be sent and summed in bfloat16 or wider, within the bound.
A program may use at most 128 MiB of HBM per device.

```python
import math
import jax
import jax.numpy as jnp
import numpy as np
from jax import lax

D = 2048
HEAD_COUNT = 32
HEAD_DIM = 64
FF = 5120
REACH = 4
TOK_DEV = 384
TOKEN_COUNT = 6144
DOCS = 8
N_TP = 2


def drawn(key):
    base_key = jax.random.fold_in(key, 11)
    key_q, key_k = jax.random.split(base_key, 2)
    col_count = HEAD_COUNT * HEAD_DIM
    queries = jax.random.normal(key_q, (TOKEN_COUNT, col_count), jnp.float32)
    keys = jax.random.normal(key_k, (TOKEN_COUNT, col_count), jnp.float32)
    return (jnp.clip(queries, -48.0, 48.0), jnp.clip(keys, -48.0, 48.0))


def draw_queries(key, part):
    return drawn(key)[0].astype(jnp.bfloat16)


def draw_keys(key, part):
    return drawn(key)[1].astype(jnp.bfloat16)


def draw_gate_cache(key, part):
    base_key = jax.random.fold_in(key, 23)
    key_h, key_r, key_s, key_b, key_u, key_position, key_document = jax.random.split(base_key, 7)
    head_order = jax.random.permutation(key_h, HEAD_COUNT)
    slow_heads = head_order < HEAD_COUNT // 2
    fast_rate = jnp.exp(jax.random.uniform(key_r, (HEAD_COUNT,), jnp.float32, math.log(1.0 / 100.0), math.log(1.0 / 30.0)))
    slow_rate = jax.random.uniform(key_s, (HEAD_COUNT,), jnp.float32, 0.5, 2.0) / TOKEN_COUNT
    head_rate = jnp.where(slow_heads, slow_rate, fast_rate)
    blocks = TOKEN_COUNT // TOK_DEV
    factor = jnp.exp(jax.random.uniform(key_b, (blocks,), jnp.float32, math.log(0.4), math.log(2.5)))
    factor_rows = jnp.repeat(factor, TOK_DEV)
    wobble = jax.random.uniform(key_u, (TOKEN_COUNT, HEAD_COUNT), jnp.float32, 0.2, 1.8)
    logarithm_gate = -head_rate[None, :] * factor_rows[:, None] * wobble
    spike_start = jax.random.randint(key_position, (8,), 0, TOKEN_COUNT)
    spike_length = jnp.log(jax.random.uniform(key_document, (8, HEAD_COUNT), jnp.float32, 0.5, 0.8))
    logarithm_gate = logarithm_gate.at[spike_start].add(spike_length)
    return jnp.cumsum(logarithm_gate, axis=0)


def block_scale(stream_key, shape, cuts, least, largest):
    def one(position, parts):
        heights = jax.random.uniform(jax.random.fold_in(jax.random.fold_in(stream_key, 6), position), (parts,), jnp.float32, least / len(cuts), largest / len(cuts))
        return jnp.repeat(jnp.exp(heights), shape[position] // parts).reshape((-1,) + (1,) * (len(shape) - position - 1))

    loudness = one(*cuts[0])
    for cut in cuts[1:]:
        loudness = loudness * one(*cut)
    return loudness


def length_profile(amount, total, limit, slope):
    portions = [(1 << 20) // math.isqrt(rank ** slope) + 1 for rank in range(2, amount + 1)]
    surplus, given = total - limit - (amount - 1), [1] * (amount - 1)
    while surplus > 0:
        candidates = [i for i in range(amount - 1) if given[i] < limit]
        whole, remaining = sum([portions[i] for i in candidates]), surplus
        for i in candidates:
            addition = min(limit - given[i], max(1, remaining * portions[i] // whole), surplus)
            given[i] = given[i] + addition
            surplus = surplus - addition
    return np.array([limit] + given)


def ragged_sizes(rng, count, total, most, slope):
    if count == 2:
        one = jax.random.randint(rng, (), max(1, total - most), min(most, total - 1) + 1)
        return jnp.stack([one, total - one])
    tallies = jnp.asarray(length_profile(count, total, most, slope), jnp.int32)
    twos = (count - 1) // 2
    source_of, taker = tallies[1:1 + 2 * twos:2], tallies[2:2 + 2 * twos:2]
    margin = jnp.minimum(source_of - 1, most - taker)
    shifted = jax.random.randint(jax.random.fold_in(rng, 1), (twos,), 0, 1 << 20) % (margin + 1)
    tallies = tallies.at[1:1 + 2 * twos:2].set(source_of - shifted).at[2:2 + 2 * twos:2].set(taker + shifted)
    return tallies[jax.random.permutation(jax.random.fold_in(rng, 2), count)]


def noise(rng, dims, scale, reach, pieces=(), held_as=jnp.bfloat16):
    level = block_scale(rng, dims, pieces, -0.22, 0.18) if pieces else 1.0
    drawn = jax.random.normal(rng, dims, jnp.float32) * scale * level
    return jnp.minimum(jnp.maximum(drawn, -reach), reach).astype(held_as)


def setup_inputs(seed: int = 0) -> dict:
    streams_of = jax.random.split(jax.random.key(seed), 12)
    return {
        "residual": noise(streams_of[0], (TOKEN_COUNT, D), 1.0, 6.0, ((0, 16),)),
        "queries": draw_queries(jax.random.fold_in(streams_of[11], 71), 0),
        "keys": draw_keys(jax.random.fold_in(streams_of[11], 71), 0),
        "values": noise(streams_of[3], (TOKEN_COUNT, HEAD_COUNT * HEAD_DIM), 1.0, 6.0, ((0, 16), (1, 2))),
        "gate_cache": draw_gate_cache(jax.random.fold_in(streams_of[11], 71), 0),
        "doc_ids": jnp.searchsorted(jnp.cumsum(ragged_sizes(streams_of[5], DOCS, TOKEN_COUNT, REACH * TOK_DEV, 0)), jnp.arange(TOKEN_COUNT), side="right").astype(jnp.int32),
        "out_weight": noise(streams_of[6], (HEAD_COUNT * HEAD_DIM, D), (HEAD_COUNT * HEAD_DIM // 64) ** -0.5, 1.0, ((0, 2),)),
        "mix_gain": jnp.clip(1.0 + 0.18 * jax.random.normal(streams_of[7], (D,), jnp.float32), 0.1, 1.9),
        "gate_weight": noise(streams_of[8], (D, FF), D ** -0.5, 0.125, ((0, 16), (1, 2))),
        "up_weight": noise(streams_of[9], (D, FF), D ** -0.5, 0.125, ((0, 16), (1, 2))),
        "down_weight": noise(streams_of[10], (FF, D), (FF // 4) ** -0.5, 0.15625, ((0, 2), (1, 16))),
    }


EPSILON = 1e-06
NEGATIVE = -1e+30

def group_sum(activations, weight, groups):
    row_count = activations.shape[0]
    inner_cols = activations.shape[1] // groups
    left_grouped = activations.reshape(row_count, groups, inner_cols).transpose(1, 0, 2)
    right_grouped = weight.reshape(groups, inner_cols, weight.shape[1])

    def add_group(running, operands):
        partial_value = jnp.dot(operands[0], operands[1], preferred_element_type=jnp.float32)
        rounded = lax.optimization_barrier(partial_value.astype(jnp.bfloat16))
        return (running + rounded.astype(jnp.float32), None)
    zeros_init = jnp.zeros((row_count, weight.shape[1]), jnp.float32)
    running, ignored = lax.scan(add_group, zeros_init, (left_grouped, right_grouped))
    return running

def normalize(middle, gain):
    widened = middle.astype(jnp.float32)
    factor = lax.rsqrt(lax.optimization_barrier(jnp.mean(widened * widened, axis=-1, keepdims=True)) + EPSILON)
    return (widened * factor * gain).astype(jnp.bfloat16)

def attend(queries, keys, values, gate_cache, doc_ids):
    tokens = queries.shape[0]
    doc_span = REACH * TOK_DEV
    block_rows = math.gcd(tokens, 512)
    key_count = doc_span + block_rows
    head_shape = (tokens, HEAD_COUNT, HEAD_DIM)
    query_heads = queries.reshape(head_shape)
    pad_rows = ((doc_span, 0), (0, 0), (0, 0))
    key_heads = jnp.pad(keys.reshape(head_shape), pad_rows)
    value_heads = jnp.pad(values.reshape(head_shape), pad_rows)
    cache_pad = jnp.pad(gate_cache, ((doc_span, 0), (0, 0)))
    docs_pad = jnp.pad(doc_ids, (doc_span, 0), constant_values=-1)
    score_scale = HEAD_DIM ** (-0.5)

    def one_block(block_index):
        start_row = (block_index * block_rows).astype(jnp.int32)
        query_block = lax.dynamic_slice_in_dim(query_heads, start_row, block_rows, 0).astype(jnp.float32)
        key_block = lax.dynamic_slice_in_dim(key_heads, start_row, key_count, 0).astype(jnp.float32)
        value_block = lax.dynamic_slice_in_dim(value_heads, start_row, key_count, 0).astype(jnp.float32)
        query_cache = lax.dynamic_slice_in_dim(gate_cache, start_row, block_rows, 0)
        key_cache = lax.dynamic_slice_in_dim(cache_pad, start_row, key_count, 0)
        query_docs = lax.dynamic_slice_in_dim(doc_ids, start_row, block_rows, 0)
        key_docs = lax.dynamic_slice_in_dim(docs_pad, start_row, key_count, 0)
        query_pos = start_row + jnp.arange(block_rows, dtype=jnp.int32)
        key_pos = start_row - doc_span + jnp.arange(key_count, dtype=jnp.int32)
        visible = (key_pos[None, :] <= query_pos[:, None]) & (key_pos[None, :] >= 0) & (key_docs[None, :] == query_docs[:, None])
        scores = jnp.einsum('qhd,khd->hqk', query_block, key_block) * score_scale
        scores = scores + query_cache.T[:, :, None] - key_cache.T[:, None, :]
        scores = jnp.where(visible[None], scores, NEGATIVE)
        row_max = lax.optimization_barrier(jnp.max(scores, axis=-1, keepdims=True))
        exp_scores = jnp.exp(scores - row_max)
        weights = (exp_scores / lax.optimization_barrier(jnp.sum(exp_scores, axis=-1, keepdims=True))).astype(jnp.bfloat16)
        weights = lax.optimization_barrier(weights)
        mixed_out = jnp.einsum('hqk,khd->qhd', weights.astype(jnp.float32), value_block)
        return mixed_out.astype(jnp.bfloat16)
    blocks = lax.map(one_block, jnp.arange(tokens // block_rows, dtype=jnp.int32))
    return blocks.reshape(tokens, HEAD_COUNT * HEAD_DIM)

def reference(residual, queries, keys, values, gate_cache, doc_ids, out_weight, mix_gain, gate_weight, up_weight, down_weight):
    attended = attend(queries, keys, values, gate_cache, doc_ids)
    projected = group_sum(attended, out_weight, N_TP)
    middle = (residual.astype(jnp.float32) + projected).astype(jnp.bfloat16)
    normed = normalize(middle, mix_gain)
    gate_proj = jnp.dot(normed, gate_weight, preferred_element_type=jnp.float32)
    up_proj = jnp.dot(normed, up_weight, preferred_element_type=jnp.float32)
    hidden = (jax.nn.silu(gate_proj) * up_proj).astype(jnp.bfloat16)
    lowered = group_sum(hidden, down_weight, N_TP)
    return (middle.astype(jnp.float32) + lowered).astype(jnp.bfloat16)
```

```python
import functools

import jax
import jax.numpy as jnp
from jax import lax
from jax.experimental import pallas as pl
from jax.experimental.pallas import tpu as pltpu
from jax.sharding import PartitionSpec as P

REACH = 4


EPSILON = 1e-06
NEGATIVE = -1e30


def from_behind(value, axis, steps):
    count = lax.axis_size(axis)
    first, last = (max(0, -steps), min(count, count - steps))
    return lax.ppermute(value, axis, [(source, source + steps) for source in range(first, last)])


def normalize(middle, gain):
    widened = middle.astype(jnp.float32)
    factor = lax.rsqrt(jnp.mean(widened * widened, axis=-1, keepdims=True) + EPSILON)
    return (widened * factor * gain).astype(jnp.bfloat16)


def plain_local(
    residual,
    queries,
    keys,
    values,
    gate_cache,
    doc_ids,
    out_weight,
    mix_gain,
    gate_weight,
    up_weight,
    down_weight,
):
    tok_rows = queries.shape[0]
    heads_here = gate_cache.shape[1]
    head_size = queries.shape[1] // heads_here
    sp_index = lax.axis_index("sp")
    key_parts = [keys]
    value_parts = [values]
    cache_parts = [gate_cache]
    doc_parts = [doc_ids]
    for distance in range(1, REACH + 1):
        moved_keys, moved_values = from_behind((keys, values), "sp", distance)
        moved_cache, moved_docs = from_behind((gate_cache, doc_ids), "sp", distance)
        key_parts.append(moved_keys)
        value_parts.append(moved_values)
        cache_parts.append(moved_cache)
        doc_parts.append(moved_docs)
    all_keys = jnp.concatenate(key_parts[::-1], axis=0)
    all_values = jnp.concatenate(value_parts[::-1], axis=0)
    all_cache = jnp.concatenate(cache_parts[::-1], axis=0)
    all_docs = jnp.concatenate(doc_parts[::-1], axis=0)
    key_count = all_keys.shape[0]
    query_pos = sp_index * tok_rows + jnp.arange(tok_rows, dtype=jnp.int32)
    key_pos = (sp_index - REACH) * tok_rows + jnp.arange(key_count, dtype=jnp.int32)
    visible = (
        (key_pos[None, :] <= query_pos[:, None])
        & (key_pos[None, :] >= 0)
        & (all_docs[None, :] == doc_ids[:, None])
    )
    query_heads = queries.reshape(tok_rows, heads_here, head_size)
    key_heads = all_keys.reshape(key_count, heads_here, head_size)
    value_heads = all_values.reshape(key_count, heads_here, head_size)
    score_scale = head_size ** (-0.5)
    scores = (
        jnp.einsum("qhd,khd->hqk", query_heads, key_heads, preferred_element_type=jnp.float32)
        * score_scale
    )
    scores = scores + gate_cache.T[:, :, None] - all_cache.T[:, None, :]
    scores = jnp.where(visible[None], scores, NEGATIVE)
    row_max = jnp.max(scores, axis=-1, keepdims=True)
    exp_scores = jnp.exp(scores - row_max)
    weights = (exp_scores / jnp.sum(exp_scores, axis=-1, keepdims=True)).astype(jnp.bfloat16)
    attended = jnp.einsum("hqk,khd->qhd", weights, value_heads, preferred_element_type=jnp.float32)
    attended = attended.astype(jnp.bfloat16).reshape(tok_rows, heads_here * head_size)
    row_share = tok_rows // lax.axis_size("tp")
    tp_index = lax.axis_index("tp")
    partial_value = jnp.dot(attended, out_weight, preferred_element_type=jnp.float32)
    attn_sum = lax.psum(partial_value.astype(jnp.bfloat16), "tp").astype(jnp.float32)
    whole_middle = (residual.astype(jnp.float32) + attn_sum).astype(jnp.bfloat16)
    mixer_in = normalize(whole_middle, mix_gain)
    middle = lax.dynamic_slice_in_dim(whole_middle, tp_index * row_share, row_share, 0)
    held_gate, held_up = (
        lax.all_gather(gate_weight, "sp", axis=0, tiled=True),
        lax.all_gather(up_weight, "sp", axis=0, tiled=True),
    )
    gate_proj = jnp.dot(mixer_in, held_gate, preferred_element_type=jnp.float32)
    up_proj = jnp.dot(mixer_in, held_up, preferred_element_type=jnp.float32)
    hidden = (jax.nn.silu(gate_proj) * up_proj).astype(jnp.bfloat16)
    partials = jnp.dot(
        hidden,
        lax.all_gather(down_weight, "sp", axis=1, tiled=True),
        preferred_element_type=jnp.float32,
    )
    down_sum = lax.psum_scatter(
        partials.astype(jnp.bfloat16), "tp", scatter_dimension=0, tiled=True
    ).astype(jnp.float32)
    return (middle.astype(jnp.float32) + down_sum).astype(jnp.bfloat16)


ROWS = 128


def attend_tile(tile, plane_index, span, head_size, queries, keys, values, aux, out):
    heads = queries.shape[1] // head_size
    q_start = pl.multiple_of(tile * ROWS, ROWS)
    window = span + ROWS
    key_aux = aux[:, pl.ds(q_start, window)]
    query_aux = jnp.transpose(aux[:, pl.ds(pl.multiple_of(q_start + span, ROWS), ROWS)])
    column = lax.broadcasted_iota(jnp.int32, (ROWS, window), 1)
    row = lax.broadcasted_iota(jnp.int32, (ROWS, window), 0)
    first = (1 - plane_index) * span - q_start
    visible = (
        (column <= row + span)
        & (column >= first)
        & (key_aux[heads : heads + 1, :] == query_aux[:, heads : heads + 1])
    )
    query = queries[pl.ds(q_start, ROWS), :] * jnp.bfloat16(head_size ** (-0.5))
    parts = []
    for head in range(heads):
        lanes = slice(head * head_size, (head + 1) * head_size)
        key = keys[pl.ds(q_start, window), lanes]
        scores = lax.dot_general(
            query[:, lanes], key, (((1,), (1,)), ((), ())), preferred_element_type=jnp.float32
        )
        scores = scores + (query_aux[:, head : head + 1] - key_aux[head : head + 1, :])
        scores = jnp.where(visible, scores, NEGATIVE)
        exp_scores = jnp.exp(scores - jnp.max(scores, axis=-1, keepdims=True))
        total = jnp.sum(exp_scores, axis=-1, keepdims=True)
        mixed = jnp.dot(
            exp_scores.astype(jnp.bfloat16),
            values[pl.ds(q_start, window), lanes],
            preferred_element_type=jnp.float32,
        )
        parts.append(mixed / total)
    out[pl.ds(q_start, ROWS), :] = jnp.concatenate(parts, axis=1).astype(jnp.bfloat16)


def layer_kernel(
    planes, head_size,
    residual, queries, keys, values, aux, out_weight, gain, gate, up, down,
    out,
    q_buf, k_buf, v_buf, aux_buf, out_buf, attended, out_w, res_buf,
    gate_all, up_all, down_all, theirs_buf, mine_buf, got, mid, tokens, hidden,
    part, pair, sums, inbox,
    a_send, a_recv, a_own, h_send, h_recv, w_send, w_recv, w_own, g_send, g_recv,
    b_send, b_recv, b_own, l_own, x_send, x_recv, n_send, n_recv, f_send, f_recv,
    p_send, p_recv, r_send, r_recv,
):
    group = REACH
    me, core = lax.axis_index("sp"), lax.axis_index("tp")
    plane, place = me // group, lax.rem(me, group)
    x, y = lax.rem(place, 2), place // 2
    low, high = lax.rem(plane, 2), plane // 2
    tok = queries.shape[0]
    cols = queries.shape[1] // group
    span = tok * group
    depth = gate.shape[0]
    width = gate.shape[1] // group
    half, features = mid.shape
    sources = 2 * planes
    MESH = pl.DeviceIdType.MESH
    other = 1 - core
    partner = {"tp": other}

    def turned(step):
        return lax.rem(x + lax.rem(step, 2), 2) + 2 * lax.rem(y + step // 2, 2)

    def in_plane(step):
        return {"sp": plane * group + turned(step)}

    def same_y(at_plane, at_x):
        return at_plane * group + 2 * y + at_x

    def target(e):
        return lax.rem(plane + e // 2, planes), lax.rem(x + e % 2, 2)

    y_neighbour = {"sp": plane * group + 2 * (1 - y) + x}
    above = {"sp": lax.rem(plane + 1, planes) * group + place}
    below = {"sp": lax.rem(plane + planes - 1, planes) * group + place}

    def member(e):
        return lax.rem(low + e // 2, 2), lax.rem(x + e % 2, 2)

    def quad(e):
        its_low, its_x = member(e)
        return {"sp": same_y(high * 2 + its_low, its_x)}

    def block(e):
        its_low, its_x = member(e)
        return its_low * 2 + its_x

    barrier = pltpu.get_barrier_semaphore()

    def greet(device):
        pl.semaphore_signal(barrier, inc=1, device_id=device, device_id_type=MESH)

    greet(partner)
    for step in range(2, group):
        greet(in_plane(step))
    for e in range(1, sources):
        greet({"sp": same_y(*target(e))})
    pl.semaphore_wait(barrier, group - 2 + sources)

    def remote(src, dst, send, recv, device):
        return pltpu.make_async_remote_copy(
            src_ref=src, dst_ref=dst, send_sem=send, recv_sem=recv,
            device_id=device, device_id_type=MESH,
        )

    def late(at_place):
        return pl.ds(pl.multiple_of(span + at_place * tok, 128), tok)

    def early(at_place):
        return pl.ds(pl.multiple_of(at_place * tok, 128), tok)

    def head_cols(index):
        return pl.ds(pl.multiple_of(index * cols, 128), cols)

    def spread(step, kinds):
        to = turned(step)
        every = (
            (keys.at[:, head_cols(to)], k_buf.at[late(place), :]),
            (values.at[:, head_cols(to)], v_buf.at[late(place), :]),
            (aux.at[to], aux_buf.at[:, late(place)]),
            (queries.at[:, head_cols(to)], q_buf.at[early(place), :]),
        )
        return [
            remote(*every[i], a_send.at[i, step], a_recv.at[i, step], in_plane(step))
            for i in kinds
        ]

    def halo(step):
        at = turned(step)
        every = (
            (k_buf.at[late(at), :], k_buf.at[early(at), :]),
            (v_buf.at[late(at), :], v_buf.at[early(at), :]),
            (aux_buf.at[:, late(at)], aux_buf.at[:, early(at)]),
        )
        if step == 0:
            own_src = (keys.at[:, head_cols(place)], values.at[:, head_cols(place)], aux.at[place])
            every = tuple((src, dst) for src, (_, dst) in zip(own_src, every))
        return [
            remote(*every[i], h_send.at[i, step], h_recv.at[i, step], above) for i in range(3)
        ]

    def halo_arrived(at):
        step = lax.rem(x + lax.rem(at, 2), 2) + 2 * lax.rem(y + at // 2, 2)
        for i, ref in enumerate((k_buf.at[early(at), :], v_buf.at[early(at), :], aux_buf.at[:, early(at)])):
            remote(ref, ref, h_send.at[i, step], h_recv.at[i, step], below).wait_recv()

    def piece(m, part_index):
        at = pl.ds(pl.multiple_of(part_index * width, 128), width)
        return down.at[at, :] if m == 2 else (gate, up)[m].at[:, at]

    def slot(m, source):
        at = pl.ds(pl.multiple_of(source * depth, 128), depth)
        return down_all.at[:, at] if m == 2 else (gate_all, up_all)[m].at[at, :]

    def weight(m, e):
        to_plane, to_x = target(e)
        index = lax.rem(to_plane, 2) * 2 + to_x
        return remote(piece(m, index), slot(m, me), w_send.at[m, e], w_recv.at[m, e],
                      {"sp": same_y(to_plane, to_x)})

    own_block = block(0)
    forward_own = [
        remote(piece(m, own_block), slot(m, me), g_send.at[m, 0], g_recv.at[m, 0], y_neighbour)
        for m in range(3)
    ]

    def pass_on(m, k):
        its_plane, dx = planes - 1 - k // 2, lax.rem(k, 2)
        e = lax.rem(plane - its_plane + planes, planes) * 2 + dx

        @pl.when(e != 0)
        def _():
            held = slot(m, same_y(its_plane, lax.rem(x + dx, 2)))
            remote(held, held, w_send.at[m, e], w_recv.at[m, e], y_neighbour).wait_recv()
            remote(held, held, g_send.at[m, e], g_recv.at[m, e], y_neighbour).start()

    def pass_range(m, first, last):
        def one(k, carry):
            pass_on(m, k)
            return carry

        lax.fori_loop(first, last, one, 0)

    def gathered(m):
        def one(e, carry):
            its_plane = lax.rem(plane - e // 2 + planes, planes)
            its_x = lax.rem(x + lax.rem(e, 2), 2)
            held = slot(m, its_plane * group + 2 * (1 - y) + its_x)
            remote(held, held, g_send.at[m, e], g_recv.at[m, e], y_neighbour).wait_recv()
            return carry

        lax.fori_loop(0, sources, one, 0)

    own = [
        pltpu.make_async_copy(keys.at[:, head_cols(place)], k_buf.at[late(place), :], a_own.at[0]),
        pltpu.make_async_copy(values.at[:, head_cols(place)], v_buf.at[late(place), :], a_own.at[1]),
        pltpu.make_async_copy(aux.at[place], aux_buf.at[:, late(place)], a_own.at[2]),
        pltpu.make_async_copy(queries.at[:, head_cols(place)], q_buf.at[early(place), :], a_own.at[3]),
    ]
    kept = [
        pltpu.make_async_copy(piece(m, own_block), slot(m, me), w_own.at[m]) for m in range(3)
    ]
    core_rows = pl.ds(pl.multiple_of(core * half, 64), half)
    loads = [
        pltpu.make_async_copy(out_weight, out_w, l_own.at[0]),
        pltpu.make_async_copy(residual.at[core_rows, :], res_buf, l_own.at[1]),
    ]
    has_above, has_below = plane < planes - 1, plane > 0

    first_kinds = {step: spread(step, (0, 1, 2)) for step in range(1, group)}
    query_kinds = {step: spread(step, (3,)) for step in range(1, group)}
    halos = {step: halo(step) for step in range(group)}
    for step in range(1, group):
        for copy in first_kinds[step]:
            copy.start()

    @pl.when(has_above)
    def _():
        for copy in halos[0]:
            copy.start()

    for step in range(1, group):
        for copy in query_kinds[step]:
            copy.start()
    for copy in own + kept + loads:
        copy.start()
    weights = {(m, e): weight(m, e) for m in range(3) for e in range(1, sources)}

    def upward(e):
        return jnp.logical_and(e // 2 > 0, plane + e // 2 < planes)

    for m in range(3):
        forward_own[m].start()
        for e in range(1, sources):
            pl.when(jnp.logical_not(upward(e)))(weights[m, e].start)

    @pl.when(plane == 0)
    def _():
        k_buf[pl.ds(0, span), :] = jnp.zeros((span, cols), jnp.bfloat16)
        v_buf[pl.ds(0, span), :] = jnp.zeros((span, cols), jnp.bfloat16)
        aux_buf[:, pl.ds(0, span)] = jnp.zeros((aux_buf.shape[0], span), jnp.float32)

    for step in range(1, group):
        for copy in first_kinds[step]:
            copy.wait_recv()

        @pl.when(has_above)
        def _():
            for copy in halos[step]:
                copy.start()

    for m in range(3):
        for e in range(2, sources):
            pl.when(upward(e))(weights[m, e].start)
    for step in range(1, group):
        for copy in query_kinds[step]:
            copy.wait_recv()
    for copy in own:
        copy.wait()

    def back(at, start):
        step = lax.rem(x + lax.rem(at, 2), 2) + 2 * lax.rem(y + at // 2, 2)
        rows = out_buf.at[early(at), :]

        @pl.when(at != place)
        def _():
            copy = remote(rows, attended.at[:, head_cols(place)], b_send.at[step], b_recv.at[step],
                          {"sp": plane * group + at})
            copy.start() if start else copy.wait_send()

        @pl.when(at == place)
        def _():
            copy = pltpu.make_async_copy(rows, attended.at[:, head_cols(place)], b_own)
            copy.start() if start else copy.wait()

    tiles = tok // ROWS
    skip = max(0, group * tiles - sources - 1)

    def rows_of(i, carry):
        at = group - 1 - i

        @pl.when(has_below)
        def _():
            halo_arrived(at)

        def one(j, inner):
            attend_tile(at * tiles + tiles - 1 - j, plane, span, head_size,
                        q_buf, k_buf, v_buf, aux_buf, out_buf)
            k = i * tiles + j - skip

            @pl.when(jnp.logical_and(k >= 0, k < sources))
            def _():
                pass_on(0, k)

            return inner

        lax.fori_loop(0, tiles, one, 0)
        back(at, True)
        return carry

    lax.fori_loop(0, group, rows_of, 0)
    pass_range(1, 0, planes)
    for step in range(1, group):
        its = attended.at[:, head_cols(turned(step))]
        remote(its, its, b_send.at[step], b_recv.at[step], in_plane(step)).wait_recv()
    back(place, False)
    for copy in loads:
        copy.wait()

    wide = 512

    def project(first_row, dst):
        def one(i, carry):
            at = pl.ds(pl.multiple_of(i * wide, wide), wide)
            dst[:, at] = jnp.dot(
                attended[pl.ds(pl.multiple_of(first_row, 64), half), :], out_w[:, at],
                preferred_element_type=jnp.float32,
            ).astype(jnp.bfloat16)
            return carry

        lax.fori_loop(0, features // wide, one, 0)

    project(other * half, theirs_buf)
    swap = remote(theirs_buf, got, x_send, x_recv, partner)
    swap.start()
    project(core * half, mine_buf)
    swap.wait_recv()
    chunk = 32

    def middle_rows(i, carry):
        at = pl.ds(pl.multiple_of(i * chunk, chunk), chunk)
        total = mine_buf[at, :].astype(jnp.float32) + got[at, :].astype(jnp.float32)
        middle = (res_buf[at, :].astype(jnp.float32) + total).astype(jnp.bfloat16)
        mid[at, :] = middle
        tokens[own_block, core, at, :] = normalize(middle, gain[...])
        return carry

    lax.fori_loop(0, half // chunk, middle_rows, 0)
    mine = tokens.at[own_block, core]
    far = {e: remote(mine, mine, f_send.at[e], f_recv.at[e], quad(e)) for e in range(1, group)}
    for e in (3, 1, 2):
        far[e].start()
    near = {}
    for e in range(group):
        held = tokens.at[block(e), core]
        near[e] = remote(held, held, n_send.at[e], n_recv.at[e], partner)
    near[0].start()
    pass_range(1, planes, sources)
    for e in range(1, group):
        far[e].wait_recv()
        near[e].start()
    for m in range(2):
        kept[m].wait()
        gathered(m)
    each = sources // group

    def gate_and_up(e, carry):
        index = lax.rem(low + e // 2, 2) * 2 + lax.rem(x + lax.rem(e, 2), 2)
        theirs = tokens.at[index, other]
        remote(theirs, theirs, n_send.at[e], n_recv.at[e], partner).wait_recv()
        rows = tokens[index].reshape(2 * half, features)
        gate_proj = jnp.dot(rows, gate_all[...], preferred_element_type=jnp.float32)
        up_proj = jnp.dot(rows, up_all[...], preferred_element_type=jnp.float32)
        hidden[index] = (gate_proj / (1.0 + jnp.exp(-gate_proj)) * up_proj).astype(jnp.bfloat16)
        pass_range(2, e * each, (e + 1) * each)
        return carry

    lax.fori_loop(0, group, gate_and_up, 0)
    kept[2].wait()
    gathered(2)
    order = (3, 1, 2, 0)
    pairs, sent = {}, {}

    def give(e):
        index = block(e)
        pairs[e].wait_recv()

        def one(i, carry):
            at = pl.ds(pl.multiple_of(i * chunk, chunk), chunk)
            both = part[index, core, at, :].astype(jnp.float32) + pair[index, at, :].astype(jnp.float32)
            sums[e, at, :] = both.astype(jnp.bfloat16)
            return carry

        lax.fori_loop(0, half // chunk, one, 0)
        sent[e] = remote(sums.at[e], inbox.at[e], r_send.at[e], r_recv.at[e], quad(e))
        sent[e].start()

    for i, e in enumerate(order):
        index = block(e)
        lowered = jnp.dot(hidden[index], down_all[...], preferred_element_type=jnp.float32)
        part[index] = lowered.astype(jnp.bfloat16).reshape(2, half, features)
        pairs[e] = remote(part.at[index, other], pair.at[index], p_send.at[e], p_recv.at[e], partner)
        pairs[e].start()
        if i > 0:
            give(order[i - 1])
    pairs[0].wait_recv()
    for e in range(1, group):
        sent[e].wait_recv()

    def last_rows(i, carry):
        at = pl.ds(pl.multiple_of(i * chunk, chunk), chunk)
        total = part[own_block, core, at, :].astype(jnp.float32)
        total = total + pair[own_block, at, :].astype(jnp.float32)
        for e in range(1, group):
            total = total + inbox[e, at, :].astype(jnp.float32)
        out[at, :] = (mid[at, :].astype(jnp.float32) + total).astype(jnp.bfloat16)
        return carry

    lax.fori_loop(0, half // chunk, last_rows, 0)

    for step in range(1, group):
        for copy in first_kinds[step] + query_kinds[step]:
            copy.wait_send()
        back(turned(step), False)

    @pl.when(has_above)
    def _():
        for step in range(group):
            for copy in halos[step]:
                copy.wait_send()

    for copy in list(weights.values()) + [swap] + list(far.values()) + list(near.values()):
        copy.wait_send()
    for copy in list(pairs.values()) + list(sent.values()):
        copy.wait_send()

    def drain(e, carry):
        for m in range(3):
            held = slot(m, me)
            remote(held, held, g_send.at[m, e], g_recv.at[m, e], y_neighbour).wait_send()
        return carry

    lax.fori_loop(0, sources, drain, 0)


def grouped_local(
    planes,
    residual, queries, keys, values, gate_cache, doc_ids,
    out_weight, mix_gain, gate_weight, up_weight, down_weight,
):
    group = REACH
    tok, all_cols = queries.shape
    features = residual.shape[1]
    heads_here = gate_cache.shape[1]
    head_size = all_cols // heads_here
    heads = heads_here // group
    rows = gate_cache.T.reshape(group, heads, tok)
    docs = jnp.broadcast_to(doc_ids.astype(jnp.float32), (group, 1, tok))
    fill = jnp.zeros((group, 7 - heads, tok), jnp.float32)
    aux = jnp.concatenate([rows, docs, fill], axis=1)
    cols, span, half = all_cols // group, tok * group, tok // 2
    width = gate_weight.shape[1] // group
    sources = 2 * planes
    sem = pltpu.SemaphoreType.DMA
    outside = pl.BlockSpec(memory_space=pltpu.HBM)
    inside = pl.BlockSpec(memory_space=pltpu.VMEM)
    bf16 = jnp.bfloat16
    four = sem((group,))
    return pl.pallas_call(
        functools.partial(layer_kernel, planes, head_size),
        out_shape=jax.ShapeDtypeStruct((half, features), bf16),
        in_specs=[outside] * 6 + [inside] + [outside] * 3,
        out_specs=inside,
        scratch_shapes=[
            pltpu.VMEM((span, cols), bf16),
            pltpu.VMEM((2 * span, cols), bf16),
            pltpu.VMEM((2 * span, cols), bf16),
            pltpu.VMEM((8, 2 * span), jnp.float32),
            pltpu.VMEM((span, cols), bf16),
            pltpu.VMEM((tok, all_cols), bf16),
            pltpu.VMEM(out_weight.shape, bf16),
            pltpu.VMEM((half, features), bf16),
            pltpu.VMEM((features, width), bf16),
            pltpu.VMEM((features, width), bf16),
            pltpu.VMEM((width, features), bf16),
            pltpu.VMEM((half, features), bf16),
            pltpu.VMEM((half, features), bf16),
            pltpu.VMEM((half, features), bf16),
            pltpu.VMEM((half, features), bf16),
            pltpu.VMEM((group, 2, half, features), bf16),
            pltpu.VMEM((group, tok, width), bf16),
            pltpu.VMEM((group, 2, half, features), bf16),
            pltpu.VMEM((group, half, features), bf16),
            pltpu.VMEM((group, half, features), bf16),
            pltpu.VMEM((group, half, features), bf16),
            sem((4, group)), sem((4, group)), sem((4,)),
            sem((3, group)), sem((3, group)),
            sem((3, sources)), sem((3, sources)), sem((3,)),
            sem((3, sources)), sem((3, sources)),
            four, four, sem, sem((2,)),
            sem, sem, four, four, four, four, four, four, four, four,
        ],
        compiler_params=pltpu.CompilerParams(
            collective_id=0, has_side_effects=True, vmem_limit_bytes=62 * 1024 * 1024
        ),
    )(
        residual, queries, keys, values, aux, out_weight, mix_gain.reshape(1, features),
        gate_weight, up_weight, down_weight,
    )


def choose(
    residual, queries, keys, values, gate_cache, doc_ids,
    out_weight, mix_gain, gate_weight, up_weight, down_weight,
):
    arrays = (
        residual, queries, keys, values, gate_cache, doc_ids,
        out_weight, mix_gain, gate_weight, up_weight, down_weight,
    )
    count, group = lax.axis_size("sp"), REACH
    planes = count // group
    heads = gate_cache.shape[1] // group
    fits = (
        count == planes * group
        and planes % 2 == 0
        and group == 4
        and lax.axis_size("tp") == 2
        and queries.shape[0] % 64 == 0
        and gate_cache.shape[1] == heads * group
        and 1 <= heads <= 7
        and queries.shape[0] % 128 == 0
        and (queries.shape[1] // group) % 128 == 0
        and gate_weight.shape[0] % 128 == 0
        and gate_weight.shape[1] % (group * 128) == 0
        and residual.shape[1] == gate_weight.shape[0] * count
        and residual.shape[1] % 512 == 0
        and queries.shape[0] * group >= 2 * planes * ROWS
    )
    return grouped_local(planes, *arrays) if fits else plain_local(*arrays)


def solution(mesh):
    return jax.shard_map(
        choose,
        mesh=mesh,
        in_specs=(
            P("sp", None),
            P("sp", "tp"),
            P("sp", "tp"),
            P("sp", "tp"),
            P("sp", "tp"),
            P("sp"),
            P("tp", None),
            P(),
            P("sp", "tp"),
            P("sp", "tp"),
            P("tp", "sp"),
        ),
        out_specs=P(("sp", "tp"), None),
        check_vma=False,
    )
```

```python
import functools

import jax
import jax.numpy as jnp
from jax import lax
from jax.experimental import pallas as pl
from jax.experimental.pallas import tpu as pltpu
from jax.sharding import PartitionSpec as P

REACH = 4


EPSILON = 1e-06
NEGATIVE = -1e30


def from_behind(value, axis, steps):
    count = lax.axis_size(axis)
    first, last = (max(0, -steps), min(count, count - steps))
    return lax.ppermute(value, axis, [(source, source + steps) for source in range(first, last)])


def normalize(middle, gain):
    widened = middle.astype(jnp.float32)
    factor = lax.rsqrt(jnp.mean(widened * widened, axis=-1, keepdims=True) + EPSILON)
    return (widened * factor * gain).astype(jnp.bfloat16)


def plain_local(
    residual,
    queries,
    keys,
    values,
    gate_cache,
    doc_ids,
    out_weight,
    mix_gain,
    gate_weight,
    up_weight,
    down_weight,
):
    tok_rows = queries.shape[0]
    heads_here = gate_cache.shape[1]
    head_size = queries.shape[1] // heads_here
    sp_index = lax.axis_index("sp")
    key_parts = [keys]
    value_parts = [values]
    cache_parts = [gate_cache]
    doc_parts = [doc_ids]
    for distance in range(1, REACH + 1):
        moved_keys, moved_values = from_behind((keys, values), "sp", distance)
        moved_cache, moved_docs = from_behind((gate_cache, doc_ids), "sp", distance)
        key_parts.append(moved_keys)
        value_parts.append(moved_values)
        cache_parts.append(moved_cache)
        doc_parts.append(moved_docs)
    all_keys = jnp.concatenate(key_parts[::-1], axis=0)
    all_values = jnp.concatenate(value_parts[::-1], axis=0)
    all_cache = jnp.concatenate(cache_parts[::-1], axis=0)
    all_docs = jnp.concatenate(doc_parts[::-1], axis=0)
    key_count = all_keys.shape[0]
    query_pos = sp_index * tok_rows + jnp.arange(tok_rows, dtype=jnp.int32)
    key_pos = (sp_index - REACH) * tok_rows + jnp.arange(key_count, dtype=jnp.int32)
    visible = (
        (key_pos[None, :] <= query_pos[:, None])
        & (key_pos[None, :] >= 0)
        & (all_docs[None, :] == doc_ids[:, None])
    )
    query_heads = queries.reshape(tok_rows, heads_here, head_size)
    key_heads = all_keys.reshape(key_count, heads_here, head_size)
    value_heads = all_values.reshape(key_count, heads_here, head_size)
    score_scale = head_size ** (-0.5)
    scores = (
        jnp.einsum("qhd,khd->hqk", query_heads, key_heads, preferred_element_type=jnp.float32)
        * score_scale
    )
    scores = scores + gate_cache.T[:, :, None] - all_cache.T[:, None, :]
    scores = jnp.where(visible[None], scores, NEGATIVE)
    row_max = jnp.max(scores, axis=-1, keepdims=True)
    exp_scores = jnp.exp(scores - row_max)
    weights = (exp_scores / jnp.sum(exp_scores, axis=-1, keepdims=True)).astype(jnp.bfloat16)
    attended = jnp.einsum("hqk,khd->qhd", weights, value_heads, preferred_element_type=jnp.float32)
    attended = attended.astype(jnp.bfloat16).reshape(tok_rows, heads_here * head_size)
    row_share = tok_rows // lax.axis_size("tp")
    tp_index = lax.axis_index("tp")
    partial_value = jnp.dot(attended, out_weight, preferred_element_type=jnp.float32)
    attn_sum = lax.psum(partial_value.astype(jnp.bfloat16), "tp").astype(jnp.float32)
    whole_middle = (residual.astype(jnp.float32) + attn_sum).astype(jnp.bfloat16)
    mixer_in = normalize(whole_middle, mix_gain)
    middle = lax.dynamic_slice_in_dim(whole_middle, tp_index * row_share, row_share, 0)
    held_gate, held_up = (
        lax.all_gather(gate_weight, "sp", axis=0, tiled=True),
        lax.all_gather(up_weight, "sp", axis=0, tiled=True),
    )
    gate_proj = jnp.dot(mixer_in, held_gate, preferred_element_type=jnp.float32)
    up_proj = jnp.dot(mixer_in, held_up, preferred_element_type=jnp.float32)
    hidden = (jax.nn.silu(gate_proj) * up_proj).astype(jnp.bfloat16)
    partials = jnp.dot(
        hidden,
        lax.all_gather(down_weight, "sp", axis=1, tiled=True),
        preferred_element_type=jnp.float32,
    )
    down_sum = lax.psum_scatter(
        partials.astype(jnp.bfloat16), "tp", scatter_dimension=0, tiled=True
    ).astype(jnp.float32)
    return (middle.astype(jnp.float32) + down_sum).astype(jnp.bfloat16)


ROWS = 128


def attend_tile(tile, plane_index, span, head_size, queries, keys, values, aux, out):
    heads = queries.shape[1] // head_size
    q_start = pl.multiple_of(tile * ROWS, ROWS)
    window = span + ROWS
    key_aux = aux[:, pl.ds(q_start, window)]
    query_aux = jnp.transpose(aux[:, pl.ds(pl.multiple_of(q_start + span, ROWS), ROWS)])
    column = lax.broadcasted_iota(jnp.int32, (ROWS, window), 1)
    row = lax.broadcasted_iota(jnp.int32, (ROWS, window), 0)
    first = (1 - plane_index) * span - q_start
    visible = (
        (column <= row + span)
        & (column >= first)
        & (key_aux[heads : heads + 1, :] == query_aux[:, heads : heads + 1])
    )
    query = queries[pl.ds(q_start, ROWS), :] * jnp.bfloat16(head_size ** (-0.5))
    parts = []
    for head in range(heads):
        lanes = slice(head * head_size, (head + 1) * head_size)
        key = keys[pl.ds(q_start, window), lanes]
        scores = lax.dot_general(
            query[:, lanes], key, (((1,), (1,)), ((), ())), preferred_element_type=jnp.float32
        )
        scores = scores + (query_aux[:, head : head + 1] - key_aux[head : head + 1, :])
        scores = jnp.where(visible, scores, NEGATIVE)
        exp_scores = jnp.exp(scores - jnp.max(scores, axis=-1, keepdims=True))
        total = jnp.sum(exp_scores, axis=-1, keepdims=True)
        mixed = jnp.dot(
            exp_scores.astype(jnp.bfloat16),
            values[pl.ds(q_start, window), lanes],
            preferred_element_type=jnp.float32,
        )
        parts.append(mixed / total)
    out[pl.ds(q_start, ROWS), :] = jnp.concatenate(parts, axis=1).astype(jnp.bfloat16)


def layer_kernel(
    planes, head_size,
    residual, queries, keys, values, aux, out_weight, gain, gate, up, down,
    out,
    q_buf, k_buf, v_buf, aux_buf, out_buf, attended, out_w, res_buf,
    gate_all, up_all, down_all, theirs_buf, mine_buf, got, mid, tokens, hidden,
    part, pair, sums, inbox,
    a_send, a_recv, a_own, h_send, h_recv, w_send, w_recv, w_own, g_send, g_recv,
    b_send, b_recv, b_own, l_own, x_send, x_recv, n_send, n_recv, f_send, f_recv,
    p_send, p_recv, r_send, r_recv,
):
    group = REACH
    me, core = lax.axis_index("sp"), lax.axis_index("tp")
    plane, place = me // group, lax.rem(me, group)
    x, y = lax.rem(place, 2), place // 2
    low, high = lax.rem(plane, 2), plane // 2
    tok = queries.shape[0]
    cols = queries.shape[1] // group
    span = tok * group
    depth = gate.shape[0]
    width = gate.shape[1] // group
    half, features = mid.shape
    sources = 2 * planes
    MESH = pl.DeviceIdType.MESH
    other = 1 - core
    partner = {"tp": other}

    def turned(step):
        return lax.rem(x + lax.rem(step, 2), 2) + 2 * lax.rem(y + step // 2, 2)

    def in_plane(step):
        return {"sp": plane * group + turned(step)}

    def same_y(at_plane, at_x):
        return at_plane * group + 2 * y + at_x

    def target(e):
        return lax.rem(plane + e // 2, planes), lax.rem(x + e % 2, 2)

    y_neighbour = {"sp": plane * group + 2 * (1 - y) + x}
    above = {"sp": lax.rem(plane + 1, planes) * group + place}
    below = {"sp": lax.rem(plane + planes - 1, planes) * group + place}

    def member(e):
        return lax.rem(low + e // 2, 2), lax.rem(x + e % 2, 2)

    def quad(e):
        its_low, its_x = member(e)
        return {"sp": same_y(high * 2 + its_low, its_x)}

    def block(e):
        its_low, its_x = member(e)
        return its_low * 2 + its_x

    barrier = pltpu.get_barrier_semaphore()

    def greet(device):
        pl.semaphore_signal(barrier, inc=1, device_id=device, device_id_type=MESH)

    greet(partner)
    for step in range(2, group):
        greet(in_plane(step))
    for e in range(1, sources):
        greet({"sp": same_y(*target(e))})
    pl.semaphore_wait(barrier, group - 2 + sources)

    def remote(src, dst, send, recv, device):
        return pltpu.make_async_remote_copy(
            src_ref=src, dst_ref=dst, send_sem=send, recv_sem=recv,
            device_id=device, device_id_type=MESH,
        )

    def late(at_place):
        return pl.ds(pl.multiple_of(span + at_place * tok, 128), tok)

    def early(at_place):
        return pl.ds(pl.multiple_of(at_place * tok, 128), tok)

    def head_cols(index):
        return pl.ds(pl.multiple_of(index * cols, 128), cols)

    def spread(step, kinds):
        to = turned(step)
        every = (
            (keys.at[:, head_cols(to)], k_buf.at[late(place), :]),
            (values.at[:, head_cols(to)], v_buf.at[late(place), :]),
            (aux.at[to], aux_buf.at[:, late(place)]),
            (queries.at[:, head_cols(to)], q_buf.at[early(place), :]),
        )
        return [
            remote(*every[i], a_send.at[i, step], a_recv.at[i, step], in_plane(step))
            for i in kinds
        ]

    def halo(step):
        at = turned(step)
        every = (
            (k_buf.at[late(at), :], k_buf.at[early(at), :]),
            (v_buf.at[late(at), :], v_buf.at[early(at), :]),
            (aux_buf.at[:, late(at)], aux_buf.at[:, early(at)]),
        )
        if step == 0:
            own_src = (keys.at[:, head_cols(place)], values.at[:, head_cols(place)], aux.at[place])
            every = tuple((src, dst) for src, (_, dst) in zip(own_src, every))
        return [
            remote(*every[i], h_send.at[i, step], h_recv.at[i, step], above) for i in range(3)
        ]

    def halo_arrived(at):
        step = lax.rem(x + lax.rem(at, 2), 2) + 2 * lax.rem(y + at // 2, 2)
        for i, ref in enumerate((k_buf.at[early(at), :], v_buf.at[early(at), :], aux_buf.at[:, early(at)])):
            remote(ref, ref, h_send.at[i, step], h_recv.at[i, step], below).wait_recv()

    def piece(m, part_index):
        at = pl.ds(pl.multiple_of(part_index * width, 128), width)
        return down.at[at, :] if m == 2 else (gate, up)[m].at[:, at]

    def slot(m, source):
        at = pl.ds(pl.multiple_of(source * depth, 128), depth)
        return down_all.at[:, at] if m == 2 else (gate_all, up_all)[m].at[at, :]

    def weight(m, e):
        to_plane, to_x = target(e)
        index = lax.rem(to_plane, 2) * 2 + to_x
        return remote(piece(m, index), slot(m, me), w_send.at[m, e], w_recv.at[m, e],
                      {"sp": same_y(to_plane, to_x)})

    own_block = block(0)
    forward_own = [
        remote(piece(m, own_block), slot(m, me), g_send.at[m, 0], g_recv.at[m, 0], y_neighbour)
        for m in range(3)
    ]

    arrivals = []
    for p in range(planes):
        over, under = range(p + 1, planes), range(p - 1, -1, -1)
        order = [(z, 0) for z in over] + [(p, 1)] + [(z, 1) for z in over]
        order += [(z, 0) for z in under] + [(z, 1) for z in under]
        arrivals.append([(p - z) % planes * 2 + dx for z, dx in order])

    def pass_on(m, i):
        e = arrivals[-1][i]
        for p in range(planes - 1):
            e = jnp.where(plane == p, arrivals[p][i], e)
        its_plane = lax.rem(plane - e // 2 + planes, planes)
        held = slot(m, same_y(its_plane, lax.rem(x + lax.rem(e, 2), 2)))
        with jax.named_scope(f"pass_{m}_{i}"):
            remote(held, held, w_send.at[m, e], w_recv.at[m, e], y_neighbour).wait_recv()
            remote(held, held, g_send.at[m, e], g_recv.at[m, e], y_neighbour).start()

    def gathered(m):
        def one(e, carry):
            its_plane = lax.rem(plane - e // 2 + planes, planes)
            its_x = lax.rem(x + lax.rem(e, 2), 2)
            held = slot(m, its_plane * group + 2 * (1 - y) + its_x)
            remote(held, held, g_send.at[m, e], g_recv.at[m, e], y_neighbour).wait_recv()
            return carry

        lax.fori_loop(0, sources, one, 0)

    own = [
        pltpu.make_async_copy(keys.at[:, head_cols(place)], k_buf.at[late(place), :], a_own.at[0]),
        pltpu.make_async_copy(values.at[:, head_cols(place)], v_buf.at[late(place), :], a_own.at[1]),
        pltpu.make_async_copy(aux.at[place], aux_buf.at[:, late(place)], a_own.at[2]),
        pltpu.make_async_copy(queries.at[:, head_cols(place)], q_buf.at[early(place), :], a_own.at[3]),
    ]
    kept = [
        pltpu.make_async_copy(piece(m, own_block), slot(m, me), w_own.at[m]) for m in range(3)
    ]
    core_rows = pl.ds(pl.multiple_of(core * half, 64), half)
    loads = [
        pltpu.make_async_copy(out_weight, out_w, l_own.at[0]),
        pltpu.make_async_copy(residual.at[core_rows, :], res_buf, l_own.at[1]),
    ]
    has_above, has_below = plane < planes - 1, plane > 0

    first_kinds = {step: spread(step, (0, 1, 2)) for step in range(1, group)}
    query_kinds = {step: spread(step, (3,)) for step in range(1, group)}
    halos = {step: halo(step) for step in range(group)}
    for step in range(1, group):
        for copy in first_kinds[step]:
            copy.start()

    @pl.when(has_above)
    def _():
        for copy in halos[0]:
            copy.start()

    for step in range(1, group):
        for copy in query_kinds[step]:
            copy.start()
    for copy in own + kept + loads:
        copy.start()
    weights = {(m, e): weight(m, e) for m in range(3) for e in range(1, sources)}

    def upward(e):
        return jnp.logical_and(e // 2 > 0, plane + e // 2 < planes)

    for m in range(3):
        forward_own[m].start()
        for e in range(2, sources, 2):
            pl.when(jnp.logical_not(upward(e)))(weights[m, e].start)

    def issue(m, going_up):
        for e in list(range(2, sources, 2)) + list(range(3, sources, 2)):
            if going_up:
                pl.when(upward(e))(weights[m, e].start)
            elif e % 2:
                pl.when(jnp.logical_not(upward(e)))(weights[m, e].start)

    @pl.when(plane == 0)
    def _():
        k_buf[pl.ds(0, span), :] = jnp.zeros((span, cols), jnp.bfloat16)
        v_buf[pl.ds(0, span), :] = jnp.zeros((span, cols), jnp.bfloat16)
        aux_buf[:, pl.ds(0, span)] = jnp.zeros((aux_buf.shape[0], span), jnp.float32)

    for at_y, steps in ((0, (2, 3, 1)), (1, (1, 2, 3))):
        @pl.when(y == at_y)
        def _():
            for step in steps:
                for copy in first_kinds[step]:
                    copy.wait_recv()

                @pl.when(has_above)
                def _():
                    for copy in halos[step]:
                        copy.start()

    weights[0, 1].start()
    weights[1, 1].start()
    issue(0, False)
    for step in range(1, group):
        for copy in query_kinds[step]:
            copy.wait_recv()
    for copy in own:
        copy.wait()

    def back(at, start):
        step = lax.rem(x + lax.rem(at, 2), 2) + 2 * lax.rem(y + at // 2, 2)
        rows = out_buf.at[early(at), :]

        @pl.when(at != place)
        def _():
            copy = remote(rows, attended.at[:, head_cols(place)], b_send.at[step], b_recv.at[step],
                          {"sp": plane * group + at})
            copy.start() if start else copy.wait_send()

        @pl.when(at == place)
        def _():
            copy = pltpu.make_async_copy(rows, attended.at[:, head_cols(place)], b_own)
            copy.start() if start else copy.wait()

    tiles = tok // ROWS
    plan = {2: (0, 0), 4: (1, 0)}
    for k in range(3):
        plan[group * tiles - 3 + k] = (0, 1 + k)

    def second():
        issue(1, True)
        issue(1, False)
        weights[2, 1].start()

    def third():
        pl.when(low == 1)(functools.partial(issue, 2, True))

    steps_of = (
        (jnp.where(core == 0, 1, 4), functools.partial(issue, 0, True)),
        (jnp.where(core == 0, 5, 8), second),
        (jnp.where(core == 0, 9, 10), third),
    )

    def rows_of(i, carry):
        at = group - 1 - i

        @pl.when(has_below)
        def _():
            with jax.named_scope("halo"):
                halo_arrived(at)

        def one(j, inner):
            attend_tile(at * tiles + tiles - 1 - j, plane, span, head_size,
                        q_buf, k_buf, v_buf, aux_buf, out_buf)
            for at_tile, (m, k) in plan.items():
                pl.when(i * tiles + j == at_tile)(functools.partial(pass_on, m, k))
            for at_tile, step in steps_of:
                pl.when(i * tiles + j == at_tile)(step)
            return inner

        lax.fori_loop(0, tiles, one, 0)
        back(at, True)
        return carry

    lax.fori_loop(0, group, rows_of, 0)
    for step in range(1, group):
        its = attended.at[:, head_cols(turned(step))]
        remote(its, its, b_send.at[step], b_recv.at[step], in_plane(step)).wait_recv()
    back(place, False)
    for copy in loads:
        copy.wait()

    wide = 512

    def project(first_row, dst):
        def one(i, carry):
            at = pl.ds(pl.multiple_of(i * wide, wide), wide)
            dst[:, at] = jnp.dot(
                attended[pl.ds(pl.multiple_of(first_row, 64), half), :], out_w[:, at],
                preferred_element_type=jnp.float32,
            ).astype(jnp.bfloat16)
            return carry

        lax.fori_loop(0, features // wide, one, 0)

    project(other * half, theirs_buf)
    swap = remote(theirs_buf, got, x_send, x_recv, partner)
    swap.start()
    project(core * half, mine_buf)
    swap.wait_recv()
    chunk = 32

    def middle_rows(i, carry):
        at = pl.ds(pl.multiple_of(i * chunk, chunk), chunk)
        total = mine_buf[at, :].astype(jnp.float32) + got[at, :].astype(jnp.float32)
        middle = (res_buf[at, :].astype(jnp.float32) + total).astype(jnp.bfloat16)
        mid[at, :] = middle
        tokens[own_block, core, at, :] = normalize(middle, gain[...])
        return carry

    lax.fori_loop(0, half // chunk, middle_rows, 0)
    part_rows = half // 2

    def shared(e, h):
        return tokens.at[block(e), core, pl.ds(h * part_rows, part_rows), :]

    def far_copy(e, h):
        if e < 3:
            return remote(shared(0, h), shared(0, h), f_send.at[e, h], f_recv.at[e, h], quad(e))
        held = shared(1 + h, h)
        return remote(held, held, f_send.at[e, h], f_recv.at[e, h], quad(2 - h))

    far = {(e, h): far_copy(e, h) for e in range(1, group) for h in range(2)}
    for e, h in ((1, 0), (2, 1), (1, 1), (2, 0)):
        far[e, h].start()
    near = {}
    for e in range(group):
        held = tokens.at[block(e), core]
        near[e] = remote(held, held, n_send.at[e], n_recv.at[e], partner)
    near[0].start()
    for k in range(4, sources - 1):
        pass_on(0, k)
    pass_on(2, 0)
    pass_on(1, 1)
    for h in range(2):
        far[1 + h, h].wait_recv()
        far[3, h].start()
    pl.when(low == 0)(functools.partial(issue, 2, True))
    issue(2, False)
    for k in range(2, sources - 1):
        pass_on(1, k)
    for e in range(1, group):
        for h in range(2):
            if (e, h) not in ((1, 0), (2, 1)):
                far[e, h].wait_recv()
        near[e].start()
    for m in range(2):
        kept[m].wait()
        gathered(m)

    def gate_and_up(e):
        index = block(e)
        theirs = tokens.at[index, other]
        remote(theirs, theirs, n_send.at[e], n_recv.at[e], partner).wait_recv()
        rows = tokens[index].reshape(2 * half, features)
        gate_proj = jnp.dot(rows, gate_all[...], preferred_element_type=jnp.float32)
        up_proj = jnp.dot(rows, up_all[...], preferred_element_type=jnp.float32)
        hidden[index] = (gate_proj / (1.0 + jnp.exp(-gate_proj)) * up_proj).astype(jnp.bfloat16)

    for e in range(group):
        gate_and_up(e)
        for k in range(1 + e, 2 + e):
            pass_on(2, k)
    for k in range(1 + group, sources - 1):
        pass_on(2, k)
    kept[2].wait()
    pairs, sent = {}, {}
    run = 2 * depth

    def columns(phase, its_plane):
        its_y = y if phase == 0 else 1 - y
        return pl.ds(pl.multiple_of(its_plane * group * depth + its_y * run, 128), run)

    def lower(phase, e):
        index = block(e)
        rows = hidden[index]
        for p in range(planes):
            lowered = jnp.dot(rows, down_all[:, columns(phase, p)], preferred_element_type=jnp.float32)
            part[phase, index, :, :, p * run : (p + 1) * run] = (
                lowered.astype(jnp.bfloat16).reshape(2, half, run)
            )
        copy = remote(part.at[phase, index, other], pair.at[phase, index],
                      p_send.at[phase, e], p_recv.at[phase, e], partner)
        copy.start()
        pairs[phase, e] = copy

    def landing(phase, e, h):
        return inbox.at[phase, e, pl.ds(h * part_rows, part_rows), :]

    def give(phase, e, h, extra=None):
        index = block(e)

        def one(i, carry):
            local = pl.ds(pl.multiple_of(i * chunk, chunk), chunk)
            at = pl.ds(pl.multiple_of(h * part_rows + i * chunk, chunk), chunk)
            both = part[phase, index, core, at, :].astype(jnp.float32)
            both = both + pair[phase, index, at, :].astype(jnp.float32)
            if extra is not None:
                both = both + extra[local, :].astype(jnp.float32)
            sums[phase, e, at, :] = both.astype(jnp.bfloat16)
            return carry

        lax.fori_loop(0, part_rows // chunk, one, 0)
        kind, to = (0, 1 + h) if e == 3 else (e, e)
        copy = remote(sums.at[phase, e, pl.ds(h * part_rows, part_rows), :], landing(phase, kind, h),
                      r_send.at[phase, kind, h], r_recv.at[phase, kind, h], quad(to))
        copy.start()
        sent[phase, e, h] = copy

    for phase in range(2):
        if phase:
            gathered(2)
        lower(phase, 3)
        lower(phase, 1)
        pairs[phase, 3].wait_recv()
        give(phase, 3, 0)
        give(phase, 3, 1)
        lower(phase, 2)
        pairs[phase, 1].wait_recv()
        give(phase, 1, 0)
        lower(phase, 0)
        pairs[phase, 2].wait_recv()
        give(phase, 2, 1)
        sent[phase, 3, 1].wait_recv()
        give(phase, 1, 1, landing(phase, 0, 1))
        sent[phase, 3, 0].wait_recv()
        give(phase, 2, 0, landing(phase, 0, 0))
    for phase in range(2):
        pairs[phase, 0].wait_recv()
        for e in (1, 2):
            for h in range(2):
                sent[phase, e, h].wait_recv()

    def last_rows(i, carry):
        at = pl.ds(pl.multiple_of(i * chunk, chunk), chunk)
        for phase in range(2):
            for p in range(planes):
                lanes = slice(p * run, (p + 1) * run)
                total = part[phase, own_block, core, at, lanes].astype(jnp.float32)
                total = total + pair[phase, own_block, at, lanes].astype(jnp.float32)
                for e in range(1, group - 1):
                    total = total + inbox[phase, e, at, lanes].astype(jnp.float32)
                cols_at = columns(phase, p)
                out[at, cols_at] = (mid[at, cols_at].astype(jnp.float32) + total).astype(jnp.bfloat16)
        return carry

    lax.fori_loop(0, half // chunk, last_rows, 0)

    for step in range(1, group):
        for copy in first_kinds[step] + query_kinds[step]:
            copy.wait_send()
        back(turned(step), False)

    @pl.when(has_above)
    def _():
        for step in range(group):
            for copy in halos[step]:
                copy.wait_send()

    for copy in list(weights.values()) + [swap] + list(far.values()) + list(near.values()):
        copy.wait_send()
    for copy in list(pairs.values()) + list(sent.values()):
        copy.wait_send()

    def drain(e, carry):
        for m in range(3):
            held = slot(m, me)
            remote(held, held, g_send.at[m, e], g_recv.at[m, e], y_neighbour).wait_send()
        return carry

    lax.fori_loop(0, sources, drain, 0)


def grouped_local(
    planes,
    residual, queries, keys, values, gate_cache, doc_ids,
    out_weight, mix_gain, gate_weight, up_weight, down_weight,
):
    group = REACH
    tok, all_cols = queries.shape
    features = residual.shape[1]
    heads_here = gate_cache.shape[1]
    head_size = all_cols // heads_here
    heads = heads_here // group
    rows = gate_cache.T.reshape(group, heads, tok)
    docs = jnp.broadcast_to(doc_ids.astype(jnp.float32), (group, 1, tok))
    fill = jnp.zeros((group, 7 - heads, tok), jnp.float32)
    aux = jnp.concatenate([rows, docs, fill], axis=1)
    cols, span, half = all_cols // group, tok * group, tok // 2
    width = gate_weight.shape[1] // group
    sources = 2 * planes
    sem = pltpu.SemaphoreType.DMA
    outside = pl.BlockSpec(memory_space=pltpu.HBM)
    inside = pl.BlockSpec(memory_space=pltpu.VMEM)
    bf16 = jnp.bfloat16
    four = sem((group,))
    return pl.pallas_call(
        functools.partial(layer_kernel, planes, head_size),
        out_shape=jax.ShapeDtypeStruct((half, features), bf16),
        in_specs=[outside] * 6 + [inside] + [outside] * 3,
        out_specs=inside,
        scratch_shapes=[
            pltpu.VMEM((span, cols), bf16),
            pltpu.VMEM((2 * span, cols), bf16),
            pltpu.VMEM((2 * span, cols), bf16),
            pltpu.VMEM((8, 2 * span), jnp.float32),
            pltpu.VMEM((span, cols), bf16),
            pltpu.VMEM((tok, all_cols), bf16),
            pltpu.VMEM(out_weight.shape, bf16),
            pltpu.VMEM((half, features), bf16),
            pltpu.VMEM((features, width), bf16),
            pltpu.VMEM((features, width), bf16),
            pltpu.VMEM((width, features), bf16),
            pltpu.VMEM((half, features), bf16),
            pltpu.VMEM((half, features), bf16),
            pltpu.VMEM((half, features), bf16),
            pltpu.VMEM((half, features), bf16),
            pltpu.VMEM((group, 2, half, features), bf16),
            pltpu.VMEM((group, tok, width), bf16),
            pltpu.VMEM((2, group, 2, half, features // 2), bf16),
            pltpu.VMEM((2, group, half, features // 2), bf16),
            pltpu.VMEM((2, group, half, features // 2), bf16),
            pltpu.VMEM((2, group - 1, half, features // 2), bf16),
            sem((4, group)), sem((4, group)), sem((4,)),
            sem((3, group)), sem((3, group)),
            sem((3, sources)), sem((3, sources)), sem((3,)),
            sem((3, sources)), sem((3, sources)),
            four, four, sem, sem((2,)),
            sem, sem, four, four, sem((group, 2)), sem((group, 2)),
            sem((2, group)), sem((2, group)), sem((2, 3, 2)), sem((2, 3, 2)),
        ],
        compiler_params=pltpu.CompilerParams(
            collective_id=0, has_side_effects=True, vmem_limit_bytes=62 * 1024 * 1024
        ),
    )(
        residual, queries, keys, values, aux, out_weight, mix_gain.reshape(1, features),
        gate_weight, up_weight, down_weight,
    )


def choose(
    residual, queries, keys, values, gate_cache, doc_ids,
    out_weight, mix_gain, gate_weight, up_weight, down_weight,
):
    arrays = (
        residual, queries, keys, values, gate_cache, doc_ids,
        out_weight, mix_gain, gate_weight, up_weight, down_weight,
    )
    count, group = lax.axis_size("sp"), REACH
    planes = count // group
    heads = gate_cache.shape[1] // group
    fits = (
        count == planes * group
        and planes % 2 == 0
        and planes == group
        and group == 4
        and lax.axis_size("tp") == 2
        and queries.shape[0] % 64 == 0
        and gate_cache.shape[1] == heads * group
        and 1 <= heads <= 7
        and queries.shape[0] % 128 == 0
        and (queries.shape[1] // group) % 128 == 0
        and gate_weight.shape[0] % 128 == 0
        and gate_weight.shape[1] % (group * 128) == 0
        and residual.shape[1] == gate_weight.shape[0] * count
        and residual.shape[1] % 512 == 0
        and queries.shape[0] * group >= 2 * planes * ROWS
    )
    return grouped_local(planes, *arrays) if fits else plain_local(*arrays)


def solution(mesh):
    return jax.shard_map(
        choose,
        mesh=mesh,
        in_specs=(
            P("sp", None),
            P("sp", "tp"),
            P("sp", "tp"),
            P("sp", "tp"),
            P("sp", "tp"),
            P("sp"),
            P("tp", None),
            P(),
            P("sp", "tp"),
            P("sp", "tp"),
            P("tp", "sp"),
        ),
        out_specs=P(("sp", "tp"), None),
        check_vma=False,
    )
```

```python
import functools

import jax
import jax.numpy as jnp
from jax import lax
from jax.experimental import pallas as pl
from jax.experimental.pallas import tpu as pltpu
from jax.sharding import PartitionSpec as P

REACH = 4


EPSILON = 1e-06
NEGATIVE = -1e30


def from_behind(value, axis, steps):
    count = lax.axis_size(axis)
    first, last = (max(0, -steps), min(count, count - steps))
    return lax.ppermute(value, axis, [(source, source + steps) for source in range(first, last)])


def normalize(middle, gain):
    widened = middle.astype(jnp.float32)
    factor = lax.rsqrt(jnp.mean(widened * widened, axis=-1, keepdims=True) + EPSILON)
    return (widened * factor * gain).astype(jnp.bfloat16)


def plain_local(
    residual,
    queries,
    keys,
    values,
    gate_cache,
    doc_ids,
    out_weight,
    mix_gain,
    gate_weight,
    up_weight,
    down_weight,
):
    tok_rows = queries.shape[0]
    heads_here = gate_cache.shape[1]
    head_size = queries.shape[1] // heads_here
    sp_index = lax.axis_index("sp")
    key_parts = [keys]
    value_parts = [values]
    cache_parts = [gate_cache]
    doc_parts = [doc_ids]
    for distance in range(1, REACH + 1):
        moved_keys, moved_values = from_behind((keys, values), "sp", distance)
        moved_cache, moved_docs = from_behind((gate_cache, doc_ids), "sp", distance)
        key_parts.append(moved_keys)
        value_parts.append(moved_values)
        cache_parts.append(moved_cache)
        doc_parts.append(moved_docs)
    all_keys = jnp.concatenate(key_parts[::-1], axis=0)
    all_values = jnp.concatenate(value_parts[::-1], axis=0)
    all_cache = jnp.concatenate(cache_parts[::-1], axis=0)
    all_docs = jnp.concatenate(doc_parts[::-1], axis=0)
    key_count = all_keys.shape[0]
    query_pos = sp_index * tok_rows + jnp.arange(tok_rows, dtype=jnp.int32)
    key_pos = (sp_index - REACH) * tok_rows + jnp.arange(key_count, dtype=jnp.int32)
    visible = (
        (key_pos[None, :] <= query_pos[:, None])
        & (key_pos[None, :] >= 0)
        & (all_docs[None, :] == doc_ids[:, None])
    )
    query_heads = queries.reshape(tok_rows, heads_here, head_size)
    key_heads = all_keys.reshape(key_count, heads_here, head_size)
    value_heads = all_values.reshape(key_count, heads_here, head_size)
    score_scale = head_size ** (-0.5)
    scores = (
        jnp.einsum("qhd,khd->hqk", query_heads, key_heads, preferred_element_type=jnp.float32)
        * score_scale
    )
    scores = scores + gate_cache.T[:, :, None] - all_cache.T[:, None, :]
    scores = jnp.where(visible[None], scores, NEGATIVE)
    row_max = jnp.max(scores, axis=-1, keepdims=True)
    exp_scores = jnp.exp(scores - row_max)
    weights = (exp_scores / jnp.sum(exp_scores, axis=-1, keepdims=True)).astype(jnp.bfloat16)
    attended = jnp.einsum("hqk,khd->qhd", weights, value_heads, preferred_element_type=jnp.float32)
    attended = attended.astype(jnp.bfloat16).reshape(tok_rows, heads_here * head_size)
    row_share = tok_rows // lax.axis_size("tp")
    tp_index = lax.axis_index("tp")
    partial_value = jnp.dot(attended, out_weight, preferred_element_type=jnp.float32)
    attn_sum = lax.psum(partial_value.astype(jnp.bfloat16), "tp").astype(jnp.float32)
    whole_middle = (residual.astype(jnp.float32) + attn_sum).astype(jnp.bfloat16)
    mixer_in = normalize(whole_middle, mix_gain)
    middle = lax.dynamic_slice_in_dim(whole_middle, tp_index * row_share, row_share, 0)
    held_gate, held_up = (
        lax.all_gather(gate_weight, "sp", axis=0, tiled=True),
        lax.all_gather(up_weight, "sp", axis=0, tiled=True),
    )
    gate_proj = jnp.dot(mixer_in, held_gate, preferred_element_type=jnp.float32)
    up_proj = jnp.dot(mixer_in, held_up, preferred_element_type=jnp.float32)
    hidden = (jax.nn.silu(gate_proj) * up_proj).astype(jnp.bfloat16)
    partials = jnp.dot(
        hidden,
        lax.all_gather(down_weight, "sp", axis=1, tiled=True),
        preferred_element_type=jnp.float32,
    )
    down_sum = lax.psum_scatter(
        partials.astype(jnp.bfloat16), "tp", scatter_dimension=0, tiled=True
    ).astype(jnp.float32)
    return (middle.astype(jnp.float32) + down_sum).astype(jnp.bfloat16)


ROWS = 128


def attend_tile(tile, plane_index, span, head_size, queries, keys, values, aux, out):
    heads = queries.shape[1] // head_size
    q_start = pl.multiple_of(tile * ROWS, ROWS)
    window = span + ROWS
    key_aux = aux[:, pl.ds(q_start, window)]
    query_aux = jnp.transpose(aux[:, pl.ds(pl.multiple_of(q_start + span, ROWS), ROWS)])
    column = lax.broadcasted_iota(jnp.int32, (ROWS, window), 1)
    row = lax.broadcasted_iota(jnp.int32, (ROWS, window), 0)
    first = (1 - plane_index) * span - q_start
    visible = (
        (column <= row + span)
        & (column >= first)
        & (key_aux[heads : heads + 1, :] == query_aux[:, heads : heads + 1])
    )
    query = queries[pl.ds(q_start, ROWS), :] * jnp.bfloat16(head_size ** (-0.5))
    parts = []
    for head in range(heads):
        lanes = slice(head * head_size, (head + 1) * head_size)
        key = keys[pl.ds(q_start, window), lanes]
        scores = lax.dot_general(
            query[:, lanes], key, (((1,), (1,)), ((), ())), preferred_element_type=jnp.float32
        )
        scores = scores + (query_aux[:, head : head + 1] - key_aux[head : head + 1, :])
        scores = jnp.where(visible, scores, NEGATIVE)
        exp_scores = jnp.exp(scores - jnp.max(scores, axis=-1, keepdims=True))
        total = jnp.sum(exp_scores, axis=-1, keepdims=True)
        mixed = jnp.dot(
            exp_scores.astype(jnp.bfloat16),
            values[pl.ds(q_start, window), lanes],
            preferred_element_type=jnp.float32,
        )
        parts.append(mixed / total)
    out[pl.ds(q_start, ROWS), :] = jnp.concatenate(parts, axis=1).astype(jnp.bfloat16)


def layer_kernel(
    planes, head_size,
    residual, queries, keys, values, cache, docs, out_weight, gain, gate, up, down,
    out,
    aux, q_buf, k_buf, v_buf, aux_buf, out_buf, attended, out_w, res_buf,
    gate_all, up_all, down_all, theirs_buf, mine_buf, got, mid, tokens, hidden,
    part, pair, sums, inbox,
    a_send, a_recv, a_own, h_send, h_recv, w_send, w_recv, w_own, g_send, g_recv,
    b_send, b_recv, b_own, l_own, x_send, x_recv, n_send, n_recv, f_send, f_recv,
    p_send, p_recv, r_send, r_recv,
):
    group = REACH
    me, core = lax.axis_index("sp"), lax.axis_index("tp")
    plane, place = me // group, lax.rem(me, group)
    x, y = lax.rem(place, 2), place // 2
    low, high = lax.rem(plane, 2), plane // 2
    tok = queries.shape[0]
    cols = queries.shape[1] // group
    span = tok * group
    depth = gate.shape[0]
    width = gate.shape[1] // group
    half, features = mid.shape
    sources = 2 * planes
    MESH = pl.DeviceIdType.MESH
    other = 1 - core
    partner = {"tp": other}

    def turned(step):
        return lax.rem(x + lax.rem(step, 2), 2) + 2 * lax.rem(y + step // 2, 2)

    def in_plane(step):
        return {"sp": plane * group + turned(step)}

    def same_y(at_plane, at_x):
        return at_plane * group + 2 * y + at_x

    def target(e):
        return lax.rem(plane + e // 2, planes), lax.rem(x + e % 2, 2)

    y_neighbour = {"sp": plane * group + 2 * (1 - y) + x}
    above = {"sp": lax.rem(plane + 1, planes) * group + place}
    below = {"sp": lax.rem(plane + planes - 1, planes) * group + place}

    def member(e):
        return lax.rem(low + e // 2, 2), lax.rem(x + e % 2, 2)

    def quad(e):
        its_low, its_x = member(e)
        return {"sp": same_y(high * 2 + its_low, its_x)}

    def block(e):
        its_low, its_x = member(e)
        return its_low * 2 + its_x

    barrier = pltpu.get_barrier_semaphore()

    def greet(device):
        pl.semaphore_signal(barrier, inc=1, device_id=device, device_id_type=MESH)

    heads = cache.shape[0] // group
    numbers = docs[...].astype(jnp.float32).reshape(1, tok)
    for index in range(group):
        aux[index, 0:heads, :] = cache[index * heads : (index + 1) * heads, :]
        aux[index, heads : heads + 1, :] = numbers
        aux[index, heads + 1 :, :] = jnp.zeros((aux.shape[1] - heads - 1, tok), jnp.float32)
    greet(partner)
    for step in range(2, group):
        greet(in_plane(step))
    for e in range(1, sources):
        greet({"sp": same_y(*target(e))})
    pl.semaphore_wait(barrier, group - 2 + sources)

    def remote(src, dst, send, recv, device):
        return pltpu.make_async_remote_copy(
            src_ref=src, dst_ref=dst, send_sem=send, recv_sem=recv,
            device_id=device, device_id_type=MESH,
        )

    def late(at_place):
        return pl.ds(pl.multiple_of(span + at_place * tok, 128), tok)

    def early(at_place):
        return pl.ds(pl.multiple_of(at_place * tok, 128), tok)

    def head_cols(index):
        return pl.ds(pl.multiple_of(index * cols, 128), cols)

    def spread(step, kinds):
        to = turned(step)
        every = (
            (keys.at[:, head_cols(to)], k_buf.at[late(place), :]),
            (values.at[:, head_cols(to)], v_buf.at[late(place), :]),
            (aux.at[to], aux_buf.at[:, late(place)]),
            (queries.at[:, head_cols(to)], q_buf.at[early(place), :]),
        )
        return [
            remote(*every[i], a_send.at[i, step], a_recv.at[i, step], in_plane(step))
            for i in kinds
        ]

    def halo(step):
        at = turned(step)
        every = (
            (k_buf.at[late(at), :], k_buf.at[early(at), :]),
            (v_buf.at[late(at), :], v_buf.at[early(at), :]),
            (aux_buf.at[:, late(at)], aux_buf.at[:, early(at)]),
        )
        if step == 0:
            own_src = (keys.at[:, head_cols(place)], values.at[:, head_cols(place)], aux.at[place])
            every = tuple((src, dst) for src, (_, dst) in zip(own_src, every))
        return [
            remote(*every[i], h_send.at[i, step], h_recv.at[i, step], above) for i in range(3)
        ]

    def halo_arrived(at):
        step = lax.rem(x + lax.rem(at, 2), 2) + 2 * lax.rem(y + at // 2, 2)
        for i, ref in enumerate((k_buf.at[early(at), :], v_buf.at[early(at), :], aux_buf.at[:, early(at)])):
            remote(ref, ref, h_send.at[i, step], h_recv.at[i, step], below).wait_recv()

    def piece(m, part_index):
        at = pl.ds(pl.multiple_of(part_index * width, 128), width)
        return down.at[at, :] if m == 2 else (gate, up)[m].at[:, at]

    def slot(m, source):
        at = pl.ds(pl.multiple_of(source * depth, 128), depth)
        return down_all.at[:, at] if m == 2 else (gate_all, up_all)[m].at[at, :]

    def weight(m, e):
        to_plane, to_x = target(e)
        index = lax.rem(to_plane, 2) * 2 + to_x
        return remote(piece(m, index), slot(m, me), w_send.at[m, e], w_recv.at[m, e],
                      {"sp": same_y(to_plane, to_x)})

    own_block = block(0)
    forward_own = [
        remote(piece(m, own_block), slot(m, me), g_send.at[m, 0], g_recv.at[m, 0], y_neighbour)
        for m in range(3)
    ]

    arrivals = []
    for p in range(planes):
        mate = p ^ 1
        over = [z for z in range(p + 1, planes) if z != mate]
        under = [z for z in range(p - 1, -1, -1) if z != mate]
        order = [(mate, 0), (p, 1)] if mate > p else [(p, 1), (mate, 0)]
        order += [(mate, 1)] + [(z, 0) for z in over] + [(z, 1) for z in over]
        order += [(z, 0) for z in under] + [(z, 1) for z in under]
        arrivals.append([(p - z) % planes * 2 + dx for z, dx in order])

    def pass_on(m, i):
        e = arrivals[-1][i]
        for p in range(planes - 1):
            e = jnp.where(plane == p, arrivals[p][i], e)
        its_plane = lax.rem(plane - e // 2 + planes, planes)
        held = slot(m, same_y(its_plane, lax.rem(x + lax.rem(e, 2), 2)))
        with jax.named_scope(f"pass_{m}_{i}"):
            remote(held, held, w_send.at[m, e], w_recv.at[m, e], y_neighbour).wait_recv()
            remote(held, held, g_send.at[m, e], g_recv.at[m, e], y_neighbour).start()

    def gathered(m, its_high):
        def one(k, carry):
            its_plane, dx = its_high * 2 + k // 2, lax.rem(k, 2)
            e = lax.rem(plane - its_plane + planes, planes) * 2 + dx
            held = slot(m, its_plane * group + 2 * (1 - y) + lax.rem(x + dx, 2))
            remote(held, held, g_send.at[m, e], g_recv.at[m, e], y_neighbour).wait_recv()
            return carry

        lax.fori_loop(0, 4, one, 0)

    own = [
        pltpu.make_async_copy(keys.at[:, head_cols(place)], k_buf.at[late(place), :], a_own.at[0]),
        pltpu.make_async_copy(values.at[:, head_cols(place)], v_buf.at[late(place), :], a_own.at[1]),
        pltpu.make_async_copy(aux.at[place], aux_buf.at[:, late(place)], a_own.at[2]),
        pltpu.make_async_copy(queries.at[:, head_cols(place)], q_buf.at[early(place), :], a_own.at[3]),
    ]
    kept = [
        pltpu.make_async_copy(piece(m, own_block), slot(m, me), w_own.at[m]) for m in range(3)
    ]
    core_rows = pl.ds(pl.multiple_of(core * half, 64), half)
    loads = [
        pltpu.make_async_copy(out_weight, out_w, l_own.at[0]),
        pltpu.make_async_copy(residual.at[core_rows, :], res_buf, l_own.at[1]),
    ]
    has_above, has_below = plane < planes - 1, plane > 0

    far_first = (3, 1, 2)
    first_kinds = {step: spread(step, (0, 1, 2)) for step in range(1, group)}
    query_kinds = {step: spread(step, (3,)) for step in range(1, group)}
    halos = {step: halo(step) for step in range(group)}
    weights = {(m, e): weight(m, e) for m in range(3) for e in range(1, sources)}

    def upward(e):
        return jnp.logical_and(e // 2 > 0, plane + e // 2 < planes)

    for step in far_first:
        for copy in first_kinds[step]:
            copy.start()
    filling = (2, 4)
    for e in filling:
        pl.when(upward(e))(weights[0, e].start)
    for step in far_first:
        for copy in query_kinds[step]:
            copy.start()
    for copy in own + kept + loads:
        copy.start()
    for m in range(3):
        forward_own[m].start()
        for e in range(2, sources, 2):
            pl.when(jnp.logical_not(upward(e)))(weights[m, e].start)

    def issue_up(m, first_e):
        for e in range(first_e, sources, 2):
            if m > 0 or e not in filling:
                pl.when(upward(e))(weights[m, e].start)

    def issue_down(m):
        for e in range(3, sources, 2):
            pl.when(jnp.logical_not(upward(e)))(weights[m, e].start)

    @pl.when(plane == 0)
    def _():
        k_buf[pl.ds(0, span), :] = jnp.zeros((span, cols), jnp.bfloat16)
        v_buf[pl.ds(0, span), :] = jnp.zeros((span, cols), jnp.bfloat16)
        aux_buf[:, pl.ds(0, span)] = jnp.zeros((aux_buf.shape[0], span), jnp.float32)

    for its_place in range(group):
        @pl.when(place == its_place)
        def _():
            for at in range(group - 1, -1, -1):
                step = its_place ^ at
                if step:
                    for copy in first_kinds[step]:
                        copy.wait_recv()

                @pl.when(has_above)
                def _():
                    for copy in halos[step]:
                        copy.start()

    for copy in own:
        copy.wait()

    def back(at, start):
        step = lax.rem(x + lax.rem(at, 2), 2) + 2 * lax.rem(y + at // 2, 2)
        rows = out_buf.at[early(at), :]

        @pl.when(at != place)
        def _():
            copy = remote(rows, attended.at[:, head_cols(place)], b_send.at[step], b_recv.at[step],
                          {"sp": plane * group + at})
            copy.start() if start else copy.wait_send()

        @pl.when(at == place)
        def _():
            copy = pltpu.make_async_copy(rows, attended.at[:, head_cols(place)], b_own)
            copy.start() if start else copy.wait()

    tiles = tok // ROWS
    last_tile = group * tiles - 1
    plan = {5: (0, 0), 6: (1, 0), last_tile - 4: (0, 1), last_tile - 2: (0, 2), last_tile: (0, 3)}

    def first():
        weights[0, 1].start()
        weights[1, 1].start()
        issue_down(0)

    def second():
        issue_up(0, 2)
        issue_up(0, 3)

    def third():
        issue_up(1, 2)
        issue_up(1, 3)
        issue_down(1)
        weights[2, 1].start()

    def fourth():
        for e in range(2, sources):
            pl.when(jnp.logical_and(low == 1, upward(e)))(weights[2, e].start)

    steps_of = (
        (jnp.where(core == 0, 3, 4), first),
        (jnp.where(core == 0, 4, 6), second),
        (jnp.where(core == 0, 6, 7), third),
        (jnp.where(core == 0, last_tile - 1, last_tile), fourth),
    )

    def rows_of(i, carry):
        at = group - 1 - i

        @pl.when(at != place)
        def _():
            rows = q_buf.at[early(at), :]
            step = lax.rem(x + lax.rem(at, 2), 2) + 2 * lax.rem(y + at // 2, 2)
            with jax.named_scope("queries"):
                remote(rows, rows, a_send.at[3, step], a_recv.at[3, step], below).wait_recv()

        @pl.when(has_below)
        def _():
            with jax.named_scope("halo"):
                halo_arrived(at)

        def one(j, inner):
            attend_tile(at * tiles + tiles - 1 - j, plane, span, head_size,
                        q_buf, k_buf, v_buf, aux_buf, out_buf)
            for at_tile, (m, k) in plan.items():
                pl.when(i * tiles + j == at_tile)(functools.partial(pass_on, m, k))
            for at_tile, step in steps_of:
                pl.when(i * tiles + j == at_tile)(step)
            return inner

        lax.fori_loop(0, tiles, one, 0)
        back(at, True)
        return carry

    lax.fori_loop(0, group, rows_of, 0)
    for step in range(1, group):
        its = attended.at[:, head_cols(turned(step))]
        remote(its, its, b_send.at[step], b_recv.at[step], in_plane(step)).wait_recv()
    back(place, False)
    for copy in loads:
        copy.wait()

    wide = 512

    def project(first_row, dst):
        def one(i, carry):
            at = pl.ds(pl.multiple_of(i * wide, wide), wide)
            dst[:, at] = jnp.dot(
                attended[pl.ds(pl.multiple_of(first_row, 64), half), :], out_w[:, at],
                preferred_element_type=jnp.float32,
            ).astype(jnp.bfloat16)
            return carry

        lax.fori_loop(0, features // wide, one, 0)

    project(other * half, theirs_buf)
    swap = remote(theirs_buf, got, x_send, x_recv, partner)
    swap.start()
    project(core * half, mine_buf)
    swap.wait_recv()
    chunk = 32

    def middle_rows(i, carry):
        at = pl.ds(pl.multiple_of(i * chunk, chunk), chunk)
        total = mine_buf[at, :].astype(jnp.float32) + got[at, :].astype(jnp.float32)
        middle = (res_buf[at, :].astype(jnp.float32) + total).astype(jnp.bfloat16)
        mid[at, :] = middle
        tokens[own_block, core, at, :] = normalize(middle, gain[...])
        return carry

    lax.fori_loop(0, half // chunk, middle_rows, 0)
    part_rows = half // 2

    def shared(e, h):
        return tokens.at[block(e), core, pl.ds(h * part_rows, part_rows), :]

    def far_copy(e, h):
        if e < 3:
            return remote(shared(0, h), shared(0, h), f_send.at[e, h], f_recv.at[e, h], quad(e))
        held = shared(1 + h, h)
        return remote(held, held, f_send.at[e, h], f_recv.at[e, h], quad(2 - h))

    far = {(e, h): far_copy(e, h) for e in range(1, group) for h in range(2)}
    for e, h in ((1, 0), (2, 1), (1, 1), (2, 0)):
        far[e, h].start()
    near = {}
    for e in range(group):
        held = tokens.at[block(e), core]
        near[e] = remote(held, held, n_send.at[e], n_recv.at[e], partner)
    near[0].start()
    for k in range(4, sources - 1):
        pass_on(0, k)
    pass_on(2, 0)
    pass_on(1, 1)
    for h in range(2):
        far[1 + h, h].wait_recv()
        far[3, h].start()
    for e in range(2, sources):
        pl.when(jnp.logical_and(low == 0, upward(e)))(weights[2, e].start)
    issue_down(2)
    for k in range(2, sources - 1):
        pass_on(1, k)
    for m in range(2):
        kept[m].wait()
        gathered(m, 0)
        gathered(m, 1)

    def gate_and_up(e):
        index = block(e)
        theirs = tokens.at[index, other]
        remote(theirs, theirs, n_send.at[e], n_recv.at[e], partner).wait_recv()
        rows = tokens[index].reshape(2 * half, features)
        gate_proj = jnp.dot(rows, gate_all[...], preferred_element_type=jnp.float32)
        up_proj = jnp.dot(rows, up_all[...], preferred_element_type=jnp.float32)
        hidden[index] = (gate_proj / (1.0 + jnp.exp(-gate_proj)) * up_proj).astype(jnp.bfloat16)

    for e in range(1, group):
        with jax.named_scope(f"far{e}"):
            for h in range(2):
                if (e, h) not in ((1, 0), (2, 1)):
                    far[e, h].wait_recv()
        near[e].start()
        gate_and_up(e - 1)
        for k in range(1, e):
            if e > 1:
                pass_on(2, 1 if e == 2 else 1 + k)
    gate_and_up(group - 1)
    pass_on(2, group)
    kept[2].wait()
    pairs, sent = {}, {}
    run = 2 * depth
    phases = 4

    def columns(phase, p):
        its_y = y if phase < 2 else 1 - y
        its_high = high if phase % 2 == 0 else 1 - high
        return pl.ds(pl.multiple_of(((its_high * 2 + p) * group + 2 * its_y) * depth, 128), run)

    def lower(phase, e):
        index = block(e)
        rows = hidden[index]
        for p in range(2):
            lowered = jnp.dot(rows, down_all[:, columns(phase, p)], preferred_element_type=jnp.float32)
            part[phase, index, :, :, p * run : (p + 1) * run] = (
                lowered.astype(jnp.bfloat16).reshape(2, half, run)
            )
        copy = remote(part.at[phase, index, other], pair.at[phase, index],
                      p_send.at[phase, e], p_recv.at[phase, e], partner)
        copy.start()
        pairs[phase, e] = copy

    def landing(phase, e, h):
        return inbox.at[phase, e, pl.ds(h * part_rows, part_rows), :]

    def give(phase, e, h, extra=None):
        index = block(e)

        def one(i, carry):
            local = pl.ds(pl.multiple_of(i * chunk, chunk), chunk)
            at = pl.ds(pl.multiple_of(h * part_rows + i * chunk, chunk), chunk)
            both = part[phase, index, core, at, :].astype(jnp.float32)
            both = both + pair[phase, index, at, :].astype(jnp.float32)
            if extra is not None:
                both = both + extra[local, :].astype(jnp.float32)
            sums[phase, e, at, :] = both.astype(jnp.bfloat16)
            return carry

        lax.fori_loop(0, part_rows // chunk, one, 0)
        kind, to = (0, 1 + h) if e == 3 else (e, e)
        copy = remote(sums.at[phase, e, pl.ds(h * part_rows, part_rows), :], landing(phase, kind, h),
                      r_send.at[phase, kind, h], r_recv.at[phase, kind, h], quad(to))
        copy.start()
        sent[phase, e, h] = copy

    def combine(phase):
        sent[phase, 3, 1].wait_recv()
        give(phase, 1, 1, landing(phase, 0, 1))
        sent[phase, 3, 0].wait_recv()
        give(phase, 2, 0, landing(phase, 0, 0))

    for phase in range(phases):
        if phase == 1:
            for k in range(1 + group, sources - 1):
                pass_on(2, k)
        if phase > 1:
            gathered(2, high if phase == 2 else 1 - high)
        for e in (3, 1, 2, 0):
            lower(phase, e)
        if phase:
            combine(phase - 1)
        for e, h in ((3, 0), (3, 1), (1, 0), (2, 1)):
            if h == 0 or e == 2:
                pairs[phase, e].wait_recv()
            give(phase, e, h)
    combine(phases - 1)
    for phase in range(phases):
        pairs[phase, 0].wait_recv()
        for e in (1, 2):
            for h in range(2):
                sent[phase, e, h].wait_recv()

    def last_rows(i, carry):
        at = pl.ds(pl.multiple_of(i * chunk, chunk), chunk)
        for phase in range(phases):
            for p in range(2):
                lanes = slice(p * run, (p + 1) * run)
                total = part[phase, own_block, core, at, lanes].astype(jnp.float32)
                total = total + pair[phase, own_block, at, lanes].astype(jnp.float32)
                for e in range(1, group - 1):
                    total = total + inbox[phase, e, at, lanes].astype(jnp.float32)
                cols_at = columns(phase, p)
                out[at, cols_at] = (mid[at, cols_at].astype(jnp.float32) + total).astype(jnp.bfloat16)
        return carry

    lax.fori_loop(0, half // chunk, last_rows, 0)

    for step in range(1, group):
        for copy in first_kinds[step] + query_kinds[step]:
            copy.wait_send()
        back(turned(step), False)

    @pl.when(has_above)
    def _():
        for step in range(group):
            for copy in halos[step]:
                copy.wait_send()

    for copy in list(weights.values()) + [swap] + list(far.values()) + list(near.values()):
        copy.wait_send()
    for copy in list(pairs.values()) + list(sent.values()):
        copy.wait_send()

    def drain(e, carry):
        for m in range(3):
            held = slot(m, me)
            remote(held, held, g_send.at[m, e], g_recv.at[m, e], y_neighbour).wait_send()
        return carry

    lax.fori_loop(0, sources, drain, 0)


def grouped_local(
    planes,
    residual, queries, keys, values, gate_cache, doc_ids,
    out_weight, mix_gain, gate_weight, up_weight, down_weight,
):
    group = REACH
    tok, all_cols = queries.shape
    features = residual.shape[1]
    heads_here = gate_cache.shape[1]
    head_size = all_cols // heads_here
    cols, span, half = all_cols // group, tok * group, tok // 2
    width = gate_weight.shape[1] // group
    sources = 2 * planes
    sem = pltpu.SemaphoreType.DMA
    outside = pl.BlockSpec(memory_space=pltpu.HBM)
    inside = pl.BlockSpec(memory_space=pltpu.VMEM)
    bf16 = jnp.bfloat16
    four = sem((group,))
    return pl.pallas_call(
        functools.partial(layer_kernel, planes, head_size),
        out_shape=jax.ShapeDtypeStruct((half, features), bf16),
        in_specs=[outside] * 4 + [inside] * 2 + [outside, inside] + [outside] * 3,
        out_specs=inside,
        scratch_shapes=[
            pltpu.VMEM((group, 8, tok), jnp.float32),
            pltpu.VMEM((span, cols), bf16),
            pltpu.VMEM((2 * span, cols), bf16),
            pltpu.VMEM((2 * span, cols), bf16),
            pltpu.VMEM((8, 2 * span), jnp.float32),
            pltpu.VMEM((span, cols), bf16),
            pltpu.VMEM((tok, all_cols), bf16),
            pltpu.VMEM(out_weight.shape, bf16),
            pltpu.VMEM((half, features), bf16),
            pltpu.VMEM((features, width), bf16),
            pltpu.VMEM((features, width), bf16),
            pltpu.VMEM((width, features), bf16),
            pltpu.VMEM((half, features), bf16),
            pltpu.VMEM((half, features), bf16),
            pltpu.VMEM((half, features), bf16),
            pltpu.VMEM((half, features), bf16),
            pltpu.VMEM((group, 2, half, features), bf16),
            pltpu.VMEM((group, tok, width), bf16),
            pltpu.VMEM((4, group, 2, half, features // 4), bf16),
            pltpu.VMEM((4, group, half, features // 4), bf16),
            pltpu.VMEM((4, group, half, features // 4), bf16),
            pltpu.VMEM((4, group - 1, half, features // 4), bf16),
            sem((4, group)), sem((4, group)), sem((4,)),
            sem((3, group)), sem((3, group)),
            sem((3, sources)), sem((3, sources)), sem((3,)),
            sem((3, sources)), sem((3, sources)),
            four, four, sem, sem((2,)),
            sem, sem, four, four, sem((group, 2)), sem((group, 2)),
            sem((4, group)), sem((4, group)), sem((4, 3, 2)), sem((4, 3, 2)),
        ],
        compiler_params=pltpu.CompilerParams(
            collective_id=0, has_side_effects=True, vmem_limit_bytes=62 * 1024 * 1024
        ),
    )(
        residual, queries, keys, values, gate_cache.T, doc_ids, out_weight,
        mix_gain.reshape(1, features),
        gate_weight, up_weight, down_weight,
    )


def choose(
    residual, queries, keys, values, gate_cache, doc_ids,
    out_weight, mix_gain, gate_weight, up_weight, down_weight,
):
    arrays = (
        residual, queries, keys, values, gate_cache, doc_ids,
        out_weight, mix_gain, gate_weight, up_weight, down_weight,
    )
    count, group = lax.axis_size("sp"), REACH
    planes = count // group
    heads = gate_cache.shape[1] // group
    fits = (
        count == planes * group
        and planes % 2 == 0
        and planes == group
        and group == 4
        and lax.axis_size("tp") == 2
        and queries.shape[0] % 64 == 0
        and gate_cache.shape[1] == heads * group
        and 1 <= heads <= 6
        and queries.shape[0] % 128 == 0
        and (queries.shape[1] // group) % 128 == 0
        and gate_weight.shape[0] % 128 == 0
        and gate_weight.shape[1] % (group * 128) == 0
        and residual.shape[1] == gate_weight.shape[0] * count
        and residual.shape[1] % 512 == 0
        and queries.shape[0] * group >= 2 * planes * ROWS
    )
    return grouped_local(planes, *arrays) if fits else plain_local(*arrays)


def solution(mesh):
    return jax.shard_map(
        choose,
        mesh=mesh,
        in_specs=(
            P("sp", None),
            P("sp", "tp"),
            P("sp", "tp"),
            P("sp", "tp"),
            P("sp", "tp"),
            P("sp"),
            P("tp", None),
            P(),
            P("sp", "tp"),
            P("sp", "tp"),
            P("tp", "sp"),
        ),
        out_specs=P(("sp", "tp"), None),
        check_vma=False,
    )
```

```python
import functools

import jax
import jax.numpy as jnp
from jax import lax
from jax.experimental import pallas as pl
from jax.experimental.pallas import tpu as pltpu
from jax.sharding import PartitionSpec as P

REACH = 4


EPSILON = 1e-06
NEGATIVE = -1e30


def from_behind(value, axis, steps):
    count = lax.axis_size(axis)
    first, last = (max(0, -steps), min(count, count - steps))
    return lax.ppermute(value, axis, [(source, source + steps) for source in range(first, last)])


def normalize(middle, gain):
    widened = middle.astype(jnp.float32)
    factor = lax.rsqrt(jnp.mean(widened * widened, axis=-1, keepdims=True) + EPSILON)
    return (widened * factor * gain).astype(jnp.bfloat16)


def plain_local(
    residual,
    queries,
    keys,
    values,
    gate_cache,
    doc_ids,
    out_weight,
    mix_gain,
    gate_weight,
    up_weight,
    down_weight,
):
    tok_rows = queries.shape[0]
    heads_here = gate_cache.shape[1]
    head_size = queries.shape[1] // heads_here
    sp_index = lax.axis_index("sp")
    key_parts = [keys]
    value_parts = [values]
    cache_parts = [gate_cache]
    doc_parts = [doc_ids]
    for distance in range(1, REACH + 1):
        moved_keys, moved_values = from_behind((keys, values), "sp", distance)
        moved_cache, moved_docs = from_behind((gate_cache, doc_ids), "sp", distance)
        key_parts.append(moved_keys)
        value_parts.append(moved_values)
        cache_parts.append(moved_cache)
        doc_parts.append(moved_docs)
    all_keys = jnp.concatenate(key_parts[::-1], axis=0)
    all_values = jnp.concatenate(value_parts[::-1], axis=0)
    all_cache = jnp.concatenate(cache_parts[::-1], axis=0)
    all_docs = jnp.concatenate(doc_parts[::-1], axis=0)
    key_count = all_keys.shape[0]
    query_pos = sp_index * tok_rows + jnp.arange(tok_rows, dtype=jnp.int32)
    key_pos = (sp_index - REACH) * tok_rows + jnp.arange(key_count, dtype=jnp.int32)
    visible = (
        (key_pos[None, :] <= query_pos[:, None])
        & (key_pos[None, :] >= 0)
        & (all_docs[None, :] == doc_ids[:, None])
    )
    query_heads = queries.reshape(tok_rows, heads_here, head_size)
    key_heads = all_keys.reshape(key_count, heads_here, head_size)
    value_heads = all_values.reshape(key_count, heads_here, head_size)
    score_scale = head_size ** (-0.5)
    scores = (
        jnp.einsum("qhd,khd->hqk", query_heads, key_heads, preferred_element_type=jnp.float32)
        * score_scale
    )
    scores = scores + gate_cache.T[:, :, None] - all_cache.T[:, None, :]
    scores = jnp.where(visible[None], scores, NEGATIVE)
    row_max = jnp.max(scores, axis=-1, keepdims=True)
    exp_scores = jnp.exp(scores - row_max)
    weights = (exp_scores / jnp.sum(exp_scores, axis=-1, keepdims=True)).astype(jnp.bfloat16)
    attended = jnp.einsum("hqk,khd->qhd", weights, value_heads, preferred_element_type=jnp.float32)
    attended = attended.astype(jnp.bfloat16).reshape(tok_rows, heads_here * head_size)
    row_share = tok_rows // lax.axis_size("tp")
    tp_index = lax.axis_index("tp")
    partial_value = jnp.dot(attended, out_weight, preferred_element_type=jnp.float32)
    attn_sum = lax.psum(partial_value.astype(jnp.bfloat16), "tp").astype(jnp.float32)
    whole_middle = (residual.astype(jnp.float32) + attn_sum).astype(jnp.bfloat16)
    mixer_in = normalize(whole_middle, mix_gain)
    middle = lax.dynamic_slice_in_dim(whole_middle, tp_index * row_share, row_share, 0)
    held_gate, held_up = (
        lax.all_gather(gate_weight, "sp", axis=0, tiled=True),
        lax.all_gather(up_weight, "sp", axis=0, tiled=True),
    )
    gate_proj = jnp.dot(mixer_in, held_gate, preferred_element_type=jnp.float32)
    up_proj = jnp.dot(mixer_in, held_up, preferred_element_type=jnp.float32)
    hidden = (jax.nn.silu(gate_proj) * up_proj).astype(jnp.bfloat16)
    partials = jnp.dot(
        hidden,
        lax.all_gather(down_weight, "sp", axis=1, tiled=True),
        preferred_element_type=jnp.float32,
    )
    down_sum = lax.psum_scatter(
        partials.astype(jnp.bfloat16), "tp", scatter_dimension=0, tiled=True
    ).astype(jnp.float32)
    return (middle.astype(jnp.float32) + down_sum).astype(jnp.bfloat16)


ROWS = 128


def attend_tile(tile, plane_index, span, head_size, queries, keys, values, aux, out):
    heads = queries.shape[1] // head_size
    q_start = pl.multiple_of(tile * ROWS, ROWS)
    window = span + ROWS
    key_aux = aux[:, pl.ds(q_start, window)]
    query_aux = jnp.transpose(aux[:, pl.ds(pl.multiple_of(q_start + span, ROWS), ROWS)])
    column = lax.broadcasted_iota(jnp.int32, (ROWS, window), 1)
    row = lax.broadcasted_iota(jnp.int32, (ROWS, window), 0)
    first = (1 - plane_index) * span - q_start
    visible = (
        (column <= row + span)
        & (column >= first)
        & (key_aux[heads : heads + 1, :] == query_aux[:, heads : heads + 1])
    )
    query = queries[pl.ds(q_start, ROWS), :] * jnp.bfloat16(head_size ** (-0.5))
    parts = []
    for head in range(heads):
        lanes = slice(head * head_size, (head + 1) * head_size)
        key = keys[pl.ds(q_start, window), lanes]
        scores = lax.dot_general(
            query[:, lanes], key, (((1,), (1,)), ((), ())), preferred_element_type=jnp.float32
        )
        scores = scores + (query_aux[:, head : head + 1] - key_aux[head : head + 1, :])
        scores = jnp.where(visible, scores, NEGATIVE)
        exp_scores = jnp.exp(scores - jnp.max(scores, axis=-1, keepdims=True))
        total = jnp.sum(exp_scores, axis=-1, keepdims=True)
        mixed = jnp.dot(
            exp_scores.astype(jnp.bfloat16),
            values[pl.ds(q_start, window), lanes],
            preferred_element_type=jnp.float32,
        )
        parts.append(mixed / total)
    out[pl.ds(q_start, ROWS), :] = jnp.concatenate(parts, axis=1).astype(jnp.bfloat16)


def layer_kernel(
    planes, head_size,
    residual, queries, keys, values, cache, docs, out_weight, gain, gate, up, down,
    out,
    aux, q_buf, k_buf, v_buf, aux_buf, out_buf, attended, out_w, res_buf,
    gate_all, up_all, down_all, theirs_buf, mine_buf, got, mid, tokens, hidden,
    part, pair, sums, inbox,
    a_send, a_recv, a_own, h_send, h_recv, w_send, w_recv, w_own, g_send, g_recv,
    b_send, b_recv, b_own, l_own, x_send, x_recv, n_send, n_recv, f_send, f_recv,
    p_send, p_recv, r_send, r_recv,
):
    group = REACH
    me, core = lax.axis_index("sp"), lax.axis_index("tp")
    plane, place = me // group, lax.rem(me, group)
    x, y = lax.rem(place, 2), place // 2
    low, high = lax.rem(plane, 2), plane // 2
    tok = queries.shape[0]
    cols = queries.shape[1] // group
    span = tok * group
    depth = gate.shape[0]
    width = gate.shape[1] // group
    half, features = mid.shape
    sources = 2 * planes
    MESH = pl.DeviceIdType.MESH
    other = 1 - core
    partner = {"tp": other}

    def turned(step):
        return lax.rem(x + lax.rem(step, 2), 2) + 2 * lax.rem(y + step // 2, 2)

    def in_plane(step):
        return {"sp": plane * group + turned(step)}

    def same_y(at_plane, at_x):
        return at_plane * group + 2 * y + at_x

    def target(e):
        return lax.rem(plane + e // 2, planes), lax.rem(x + e % 2, 2)

    y_neighbour = {"sp": plane * group + 2 * (1 - y) + x}
    above = {"sp": lax.rem(plane + 1, planes) * group + place}
    below = {"sp": lax.rem(plane + planes - 1, planes) * group + place}

    def member(e):
        return lax.rem(low + e // 2, 2), lax.rem(x + e % 2, 2)

    def quad(e):
        its_low, its_x = member(e)
        return {"sp": same_y(high * 2 + its_low, its_x)}

    def block(e):
        its_low, its_x = member(e)
        return its_low * 2 + its_x

    barrier = pltpu.get_barrier_semaphore()

    def greet(device):
        pl.semaphore_signal(barrier, inc=1, device_id=device, device_id_type=MESH)

    heads = cache.shape[0] // group
    numbers = docs[...].astype(jnp.float32).reshape(1, tok)
    for index in range(group):
        aux[index, 0:heads, :] = cache[index * heads : (index + 1) * heads, :]
        aux[index, heads : heads + 1, :] = numbers
        aux[index, heads + 1 :, :] = jnp.zeros((aux.shape[1] - heads - 1, tok), jnp.float32)
    greet(partner)
    for step in range(2, group):
        greet(in_plane(step))
    for e in range(1, sources):
        greet({"sp": same_y(*target(e))})
    pl.semaphore_wait(barrier, group - 2 + sources)

    def remote(src, dst, send, recv, device):
        return pltpu.make_async_remote_copy(
            src_ref=src, dst_ref=dst, send_sem=send, recv_sem=recv,
            device_id=device, device_id_type=MESH,
        )

    def late(at_place):
        return pl.ds(pl.multiple_of(span + at_place * tok, 128), tok)

    def early(at_place):
        return pl.ds(pl.multiple_of(at_place * tok, 128), tok)

    def head_cols(index):
        return pl.ds(pl.multiple_of(index * cols, 128), cols)

    def spread(step, kinds):
        to = turned(step)
        every = (
            (keys.at[:, head_cols(to)], k_buf.at[late(place), :]),
            (values.at[:, head_cols(to)], v_buf.at[late(place), :]),
            (aux.at[to], aux_buf.at[:, late(place)]),
            (queries.at[:, head_cols(to)], q_buf.at[early(place), :]),
        )
        return [
            remote(*every[i], a_send.at[i, step], a_recv.at[i, step], in_plane(step))
            for i in kinds
        ]

    def halo(step):
        at = turned(step)
        every = (
            (k_buf.at[late(at), :], k_buf.at[early(at), :]),
            (v_buf.at[late(at), :], v_buf.at[early(at), :]),
            (aux_buf.at[:, late(at)], aux_buf.at[:, early(at)]),
        )
        if step == 0:
            own_src = (keys.at[:, head_cols(place)], values.at[:, head_cols(place)], aux.at[place])
            every = tuple((src, dst) for src, (_, dst) in zip(own_src, every))
        return [
            remote(*every[i], h_send.at[i, step], h_recv.at[i, step], above) for i in range(3)
        ]

    def halo_arrived(at):
        step = lax.rem(x + lax.rem(at, 2), 2) + 2 * lax.rem(y + at // 2, 2)
        for i, ref in enumerate((k_buf.at[early(at), :], v_buf.at[early(at), :], aux_buf.at[:, early(at)])):
            remote(ref, ref, h_send.at[i, step], h_recv.at[i, step], below).wait_recv()

    def piece(m, part_index):
        at = pl.ds(pl.multiple_of(part_index * width, 128), width)
        return down.at[at, :] if m == 2 else (gate, up)[m].at[:, at]

    def slot(m, source):
        at = pl.ds(pl.multiple_of(source * depth, 128), depth)
        return down_all.at[:, at] if m == 2 else (gate_all, up_all)[m].at[at, :]

    def weight(m, e):
        to_plane, to_x = target(e)
        index = lax.rem(to_plane, 2) * 2 + to_x
        return remote(piece(m, index), slot(m, me), w_send.at[m, e], w_recv.at[m, e],
                      {"sp": same_y(to_plane, to_x)})

    own_block = block(0)
    forward_own = [
        remote(piece(m, own_block), slot(m, me), g_send.at[m, 0], g_recv.at[m, 0], y_neighbour)
        for m in range(3)
    ]

    arrivals = []
    for p in range(planes):
        mate = p ^ 1
        over = [z for z in range(p + 1, planes) if z != mate]
        under = [z for z in range(p - 1, -1, -1) if z != mate]
        order = [(mate, 0), (p, 1)] if mate > p else [(p, 1), (mate, 0)]
        order += [(mate, 1)] + [(z, 0) for z in over] + [(z, 1) for z in over]
        order += [(z, 0) for z in under] + [(z, 1) for z in under]
        arrivals.append([(p - z) % planes * 2 + dx for z, dx in order])

    def pass_on(m, i):
        e = arrivals[-1][i]
        for p in range(planes - 1):
            e = jnp.where(plane == p, arrivals[p][i], e)
        its_plane = lax.rem(plane - e // 2 + planes, planes)
        held = slot(m, same_y(its_plane, lax.rem(x + lax.rem(e, 2), 2)))
        with jax.named_scope(f"pass_{m}_{i}"):
            remote(held, held, w_send.at[m, e], w_recv.at[m, e], y_neighbour).wait_recv()
            remote(held, held, g_send.at[m, e], g_recv.at[m, e], y_neighbour).start()

    def gathered(m, its_high):
        def one(k, carry):
            its_plane, dx = its_high * 2 + k // 2, lax.rem(k, 2)
            e = lax.rem(plane - its_plane + planes, planes) * 2 + dx
            held = slot(m, its_plane * group + 2 * (1 - y) + lax.rem(x + dx, 2))
            remote(held, held, g_send.at[m, e], g_recv.at[m, e], y_neighbour).wait_recv()
            return carry

        lax.fori_loop(0, 4, one, 0)

    own = [
        pltpu.make_async_copy(keys.at[:, head_cols(place)], k_buf.at[late(place), :], a_own.at[0]),
        pltpu.make_async_copy(values.at[:, head_cols(place)], v_buf.at[late(place), :], a_own.at[1]),
        pltpu.make_async_copy(aux.at[place], aux_buf.at[:, late(place)], a_own.at[2]),
        pltpu.make_async_copy(queries.at[:, head_cols(place)], q_buf.at[early(place), :], a_own.at[3]),
    ]
    kept = [
        pltpu.make_async_copy(piece(m, own_block), slot(m, me), w_own.at[m]) for m in range(3)
    ]
    core_rows = pl.ds(pl.multiple_of(core * half, 64), half)
    loads = [
        pltpu.make_async_copy(out_weight, out_w, l_own.at[0]),
        pltpu.make_async_copy(residual.at[core_rows, :], res_buf, l_own.at[1]),
    ]
    has_above, has_below = plane < planes - 1, plane > 0

    far_first = (3, 1, 2)
    first_kinds = {step: spread(step, (0, 1, 2)) for step in range(1, group)}
    query_kinds = {step: spread(step, (3,)) for step in range(1, group)}
    halos = {step: halo(step) for step in range(group)}
    weights = {(m, e): weight(m, e) for m in range(3) for e in range(1, sources)}

    def upward(e):
        return jnp.logical_and(e // 2 > 0, plane + e // 2 < planes)

    for step in far_first:
        for copy in first_kinds[step]:
            copy.start()
    filling = (2, 4)
    for e in filling:
        pl.when(upward(e))(weights[0, e].start)
    for step in far_first:
        for copy in query_kinds[step]:
            copy.start()
    for copy in own + kept + loads:
        copy.start()
    for m in range(3):
        forward_own[m].start()
        for e in range(2, sources, 2):
            pl.when(jnp.logical_not(upward(e)))(weights[m, e].start)

    def issue_up(m, first_e):
        for e in range(first_e, sources, 2):
            if m > 0 or e not in filling:
                pl.when(upward(e))(weights[m, e].start)

    def issue_down(m):
        for e in range(3, sources, 2):
            pl.when(jnp.logical_not(upward(e)))(weights[m, e].start)

    @pl.when(plane == 0)
    def _():
        k_buf[pl.ds(0, span), :] = jnp.zeros((span, cols), jnp.bfloat16)
        v_buf[pl.ds(0, span), :] = jnp.zeros((span, cols), jnp.bfloat16)
        aux_buf[:, pl.ds(0, span)] = jnp.zeros((aux_buf.shape[0], span), jnp.float32)

    for its_place in range(group):
        @pl.when(place == its_place)
        def _():
            for at in range(group - 1, -1, -1):
                step = its_place ^ at
                if step:
                    for copy in first_kinds[step]:
                        copy.wait_recv()

                @pl.when(has_above)
                def _():
                    for copy in halos[step]:
                        copy.start()

    for copy in own:
        copy.wait()

    def back(at, start):
        step = lax.rem(x + lax.rem(at, 2), 2) + 2 * lax.rem(y + at // 2, 2)
        rows = out_buf.at[early(at), :]

        @pl.when(at != place)
        def _():
            copy = remote(rows, attended.at[:, head_cols(place)], b_send.at[step], b_recv.at[step],
                          {"sp": plane * group + at})
            copy.start() if start else copy.wait_send()

        @pl.when(at == place)
        def _():
            copy = pltpu.make_async_copy(rows, attended.at[:, head_cols(place)], b_own)
            copy.start() if start else copy.wait()

    tiles = tok // ROWS
    last_tile = group * tiles - 1
    plan = {5: (0, 0), 6: (1, 0), last_tile - 4: (0, 1), last_tile - 2: (0, 2), last_tile: (0, 3)}

    def first():
        weights[0, 1].start()
        weights[1, 1].start()
        issue_down(0)

    def second():
        issue_up(0, 2)
        issue_up(0, 3)

    def third():
        issue_up(1, 2)
        issue_up(1, 3)
        weights[2, 1].start()

    def fourth():
        for e in range(2, sources):
            pl.when(jnp.logical_and(low == 1, upward(e)))(weights[2, e].start)

    steps_of = (
        (jnp.where(core == 0, 3, 4), first),
        (jnp.where(core == 0, 4, 6), second),
        (jnp.where(core == 0, 5, 6), third),
        (jnp.where(core == 0, last_tile - 1, last_tile), fourth),
    )

    def rows_of(i, carry):
        at = group - 1 - i

        @pl.when(at != place)
        def _():
            rows = q_buf.at[early(at), :]
            step = lax.rem(x + lax.rem(at, 2), 2) + 2 * lax.rem(y + at // 2, 2)
            with jax.named_scope("queries"):
                remote(rows, rows, a_send.at[3, step], a_recv.at[3, step], below).wait_recv()

        @pl.when(has_below)
        def _():
            with jax.named_scope("halo"):
                halo_arrived(at)

        def one(j, inner):
            attend_tile(at * tiles + tiles - 1 - j, plane, span, head_size,
                        q_buf, k_buf, v_buf, aux_buf, out_buf)
            for at_tile, (m, k) in plan.items():
                pl.when(i * tiles + j == at_tile)(functools.partial(pass_on, m, k))
            for at_tile, step in steps_of:
                pl.when(i * tiles + j == at_tile)(step)
            return inner

        lax.fori_loop(0, tiles, one, 0)
        back(at, True)
        return carry

    lax.fori_loop(0, group, rows_of, 0)
    issue_down(1)
    for step in range(1, group):
        its = attended.at[:, head_cols(turned(step))]
        remote(its, its, b_send.at[step], b_recv.at[step], in_plane(step)).wait_recv()
    back(place, False)
    for copy in loads:
        copy.wait()

    wide = 512

    def project(first_row, dst):
        def one(i, carry):
            at = pl.ds(pl.multiple_of(i * wide, wide), wide)
            dst[:, at] = jnp.dot(
                attended[pl.ds(pl.multiple_of(first_row, 64), half), :], out_w[:, at],
                preferred_element_type=jnp.float32,
            ).astype(jnp.bfloat16)
            return carry

        lax.fori_loop(0, features // wide, one, 0)

    project(other * half, theirs_buf)
    swap = remote(theirs_buf, got, x_send, x_recv, partner)
    swap.start()
    project(core * half, mine_buf)
    swap.wait_recv()
    chunk = 32

    def middle_rows(i, carry):
        at = pl.ds(pl.multiple_of(i * chunk, chunk), chunk)
        total = mine_buf[at, :].astype(jnp.float32) + got[at, :].astype(jnp.float32)
        middle = (res_buf[at, :].astype(jnp.float32) + total).astype(jnp.bfloat16)
        mid[at, :] = middle
        tokens[own_block, core, at, :] = normalize(middle, gain[...])
        return carry

    lax.fori_loop(0, half // chunk, middle_rows, 0)
    part_rows = half // 2

    def shared(e, h):
        return tokens.at[block(e), core, pl.ds(h * part_rows, part_rows), :]

    def far_copy(e, h):
        if e < 3:
            return remote(shared(0, h), shared(0, h), f_send.at[e, h], f_recv.at[e, h], quad(e))
        held = shared(1 + h, h)
        return remote(held, held, f_send.at[e, h], f_recv.at[e, h], quad(2 - h))

    far = {(e, h): far_copy(e, h) for e in range(1, group) for h in range(2)}
    for e, h in ((1, 0), (2, 1), (1, 1), (2, 0)):
        far[e, h].start()
    near = {}
    for e in range(group):
        held = tokens.at[block(e), core]
        near[e] = remote(held, held, n_send.at[e], n_recv.at[e], partner)
    near[0].start()
    for k in range(4, sources - 1):
        pass_on(0, k)
    pass_on(2, 0)
    for k in range(1, 5):
        pass_on(1, k)
    for h in range(2):
        far[1 + h, h].wait_recv()
        far[3, h].start()
    for e in range(2, sources):
        pl.when(jnp.logical_and(low == 0, upward(e)))(weights[2, e].start)
    issue_down(2)
    for k in range(5, sources - 1):
        pass_on(1, k)
    for m in range(2):
        kept[m].wait()
        gathered(m, 0)
        gathered(m, 1)

    def gate_and_up(e):
        index = block(e)
        theirs = tokens.at[index, other]
        remote(theirs, theirs, n_send.at[e], n_recv.at[e], partner).wait_recv()
        rows = tokens[index].reshape(2 * half, features)
        gate_proj = jnp.dot(rows, gate_all[...], preferred_element_type=jnp.float32)
        up_proj = jnp.dot(rows, up_all[...], preferred_element_type=jnp.float32)
        hidden[index] = (gate_proj / (1.0 + jnp.exp(-gate_proj)) * up_proj).astype(jnp.bfloat16)

    for e in range(1, group):
        with jax.named_scope(f"far{e}"):
            for h in range(2):
                if (e, h) not in ((1, 0), (2, 1)):
                    far[e, h].wait_recv()
        near[e].start()
        gate_and_up(e - 1)
        for k in range(1, e):
            if e > 1:
                pass_on(2, 1 if e == 2 else 1 + k)
    gate_and_up(group - 1)
    pass_on(2, group)
    kept[2].wait()
    pairs, sent = {}, {}
    run = 2 * depth
    phases = 4

    def columns(phase, p):
        its_y = y if phase < 2 else 1 - y
        its_high = high if phase % 2 == 0 else 1 - high
        return pl.ds(pl.multiple_of(((its_high * 2 + p) * group + 2 * its_y) * depth, 128), run)

    def lower(phase, e):
        index = block(e)
        rows = hidden[index]
        for p in range(2):
            lowered = jnp.dot(rows, down_all[:, columns(phase, p)], preferred_element_type=jnp.float32)
            part[phase, index, :, :, p * run : (p + 1) * run] = (
                lowered.astype(jnp.bfloat16).reshape(2, half, run)
            )
        copy = remote(part.at[phase, index, other], pair.at[phase, index],
                      p_send.at[phase, e], p_recv.at[phase, e], partner)
        copy.start()
        pairs[phase, e] = copy

    def landing(phase, e, h):
        return inbox.at[phase, e, pl.ds(h * part_rows, part_rows), :]

    def give(phase, e, h, extra=None):
        index = block(e)

        def one(i, carry):
            local = pl.ds(pl.multiple_of(i * chunk, chunk), chunk)
            at = pl.ds(pl.multiple_of(h * part_rows + i * chunk, chunk), chunk)
            both = part[phase, index, core, at, :].astype(jnp.float32)
            both = both + pair[phase, index, at, :].astype(jnp.float32)
            if extra is not None:
                both = both + extra[local, :].astype(jnp.float32)
            sums[phase, e, at, :] = both.astype(jnp.bfloat16)
            return carry

        lax.fori_loop(0, part_rows // chunk, one, 0)
        kind, to = (0, 1 + h) if e == 3 else (e, e)
        copy = remote(sums.at[phase, e, pl.ds(h * part_rows, part_rows), :], landing(phase, kind, h),
                      r_send.at[phase, kind, h], r_recv.at[phase, kind, h], quad(to))
        copy.start()
        sent[phase, e, h] = copy

    def combine(phase):
        sent[phase, 3, 1].wait_recv()
        give(phase, 1, 1, landing(phase, 0, 1))
        sent[phase, 3, 0].wait_recv()
        give(phase, 2, 0, landing(phase, 0, 0))

    for phase in range(phases):
        if phase == 1:
            for k in range(1 + group, sources - 1):
                pass_on(2, k)
        if phase > 1:
            gathered(2, high if phase == 2 else 1 - high)
        for e in (3, 1, 2, 0):
            lower(phase, e)
        if phase:
            combine(phase - 1)
        for e, h in ((3, 0), (3, 1), (1, 0), (2, 1)):
            if h == 0 or e == 2:
                pairs[phase, e].wait_recv()
            give(phase, e, h)
    combine(phases - 1)
    for phase in range(phases):
        pairs[phase, 0].wait_recv()
        for e in (1, 2):
            for h in range(2):
                sent[phase, e, h].wait_recv()

    def last_rows(i, carry):
        at = pl.ds(pl.multiple_of(i * chunk, chunk), chunk)
        for phase in range(phases):
            for p in range(2):
                lanes = slice(p * run, (p + 1) * run)
                total = part[phase, own_block, core, at, lanes].astype(jnp.float32)
                total = total + pair[phase, own_block, at, lanes].astype(jnp.float32)
                for e in range(1, group - 1):
                    total = total + inbox[phase, e, at, lanes].astype(jnp.float32)
                cols_at = columns(phase, p)
                out[at, cols_at] = (mid[at, cols_at].astype(jnp.float32) + total).astype(jnp.bfloat16)
        return carry

    lax.fori_loop(0, half // chunk, last_rows, 0)

    for step in range(1, group):
        for copy in first_kinds[step] + query_kinds[step]:
            copy.wait_send()
        back(turned(step), False)

    @pl.when(has_above)
    def _():
        for step in range(group):
            for copy in halos[step]:
                copy.wait_send()

    for copy in list(weights.values()) + [swap] + list(far.values()) + list(near.values()):
        copy.wait_send()
    for copy in list(pairs.values()) + list(sent.values()):
        copy.wait_send()

    def drain(e, carry):
        for m in range(3):
            held = slot(m, me)
            remote(held, held, g_send.at[m, e], g_recv.at[m, e], y_neighbour).wait_send()
        return carry

    lax.fori_loop(0, sources, drain, 0)


def grouped_local(
    planes,
    residual, queries, keys, values, gate_cache, doc_ids,
    out_weight, mix_gain, gate_weight, up_weight, down_weight,
):
    group = REACH
    tok, all_cols = queries.shape
    features = residual.shape[1]
    heads_here = gate_cache.shape[1]
    head_size = all_cols // heads_here
    cols, span, half = all_cols // group, tok * group, tok // 2
    width = gate_weight.shape[1] // group
    sources = 2 * planes
    sem = pltpu.SemaphoreType.DMA
    outside = pl.BlockSpec(memory_space=pltpu.HBM)
    inside = pl.BlockSpec(memory_space=pltpu.VMEM)
    bf16 = jnp.bfloat16
    four = sem((group,))
    return pl.pallas_call(
        functools.partial(layer_kernel, planes, head_size),
        out_shape=jax.ShapeDtypeStruct((half, features), bf16),
        in_specs=[outside] * 4 + [inside] * 2 + [outside, inside] + [outside] * 3,
        out_specs=inside,
        scratch_shapes=[
            pltpu.VMEM((group, 8, tok), jnp.float32),
            pltpu.VMEM((span, cols), bf16),
            pltpu.VMEM((2 * span, cols), bf16),
            pltpu.VMEM((2 * span, cols), bf16),
            pltpu.VMEM((8, 2 * span), jnp.float32),
            pltpu.VMEM((span, cols), bf16),
            pltpu.VMEM((tok, all_cols), bf16),
            pltpu.VMEM(out_weight.shape, bf16),
            pltpu.VMEM((half, features), bf16),
            pltpu.VMEM((features, width), bf16),
            pltpu.VMEM((features, width), bf16),
            pltpu.VMEM((width, features), bf16),
            pltpu.VMEM((half, features), bf16),
            pltpu.VMEM((half, features), bf16),
            pltpu.VMEM((half, features), bf16),
            pltpu.VMEM((half, features), bf16),
            pltpu.VMEM((group, 2, half, features), bf16),
            pltpu.VMEM((group, tok, width), bf16),
            pltpu.VMEM((4, group, 2, half, features // 4), bf16),
            pltpu.VMEM((4, group, half, features // 4), bf16),
            pltpu.VMEM((4, group, half, features // 4), bf16),
            pltpu.VMEM((4, group - 1, half, features // 4), bf16),
            sem((4, group)), sem((4, group)), sem((4,)),
            sem((3, group)), sem((3, group)),
            sem((3, sources)), sem((3, sources)), sem((3,)),
            sem((3, sources)), sem((3, sources)),
            four, four, sem, sem((2,)),
            sem, sem, four, four, sem((group, 2)), sem((group, 2)),
            sem((4, group)), sem((4, group)), sem((4, 3, 2)), sem((4, 3, 2)),
        ],
        compiler_params=pltpu.CompilerParams(
            collective_id=0, has_side_effects=True, vmem_limit_bytes=62 * 1024 * 1024
        ),
    )(
        residual, queries, keys, values, gate_cache.T, doc_ids, out_weight,
        mix_gain.reshape(1, features),
        gate_weight, up_weight, down_weight,
    )


def choose(
    residual, queries, keys, values, gate_cache, doc_ids,
    out_weight, mix_gain, gate_weight, up_weight, down_weight,
):
    arrays = (
        residual, queries, keys, values, gate_cache, doc_ids,
        out_weight, mix_gain, gate_weight, up_weight, down_weight,
    )
    count, group = lax.axis_size("sp"), REACH
    planes = count // group
    heads = gate_cache.shape[1] // group
    fits = (
        count == planes * group
        and planes % 2 == 0
        and planes == group
        and group == 4
        and lax.axis_size("tp") == 2
        and queries.shape[0] % 64 == 0
        and gate_cache.shape[1] == heads * group
        and 1 <= heads <= 6
        and queries.shape[0] % 128 == 0
        and (queries.shape[1] // group) % 128 == 0
        and gate_weight.shape[0] % 128 == 0
        and gate_weight.shape[1] % (group * 128) == 0
        and residual.shape[1] == gate_weight.shape[0] * count
        and residual.shape[1] % 512 == 0
        and queries.shape[0] * group >= 2 * planes * ROWS
    )
    return grouped_local(planes, *arrays) if fits else plain_local(*arrays)


def solution(mesh):
    return jax.shard_map(
        choose,
        mesh=mesh,
        in_specs=(
            P("sp", None),
            P("sp", "tp"),
            P("sp", "tp"),
            P("sp", "tp"),
            P("sp", "tp"),
            P("sp"),
            P("tp", None),
            P(),
            P("sp", "tp"),
            P("sp", "tp"),
            P("tp", "sp"),
        ),
        out_specs=P(("sp", "tp"), None),
        check_vma=False,
    )
```
